512 devices in a mesh: sp: 64 (over z, y), dp: 8 (over x, core).
Axes of the slice: x: 4, y: 8, z: 8, core: 2. Of those that a mesh axis runs over, the one named last changes fastest.
Arguments:
- tokens: bfloat16 [8192, 2048], P('sp', 'dp'), may hold values from -6 to 6
- cotangent: bfloat16 [8192, 2048], P('sp', 'dp'), may hold values from -6 to 6
- in_weight: bfloat16 [1024, 2048], P('sp', 'dp'), may hold values from -0.125 to 0.125
- out_weight: bfloat16 [1024, 2048], P('sp', 'dp'), may hold values from -0.1875 to 0.1875
- decay_rate: float32 [64, 32], P('sp'), may hold values from 0 to 1
- frequency: float32 [64, 32], P('sp'), may hold values from 4 to 40
- step_log: float32 [64], P('sp'), may hold values from -2.6593 to -1.9661
- drive_real: float32 [64, 32, 16], P('sp'), may hold values from -6 to 6
- drive_imag: float32 [64, 32, 16], P('sp'), may hold values from -6 to 6
- readout_real_part: float32 [64, 16, 32], P('sp'), may hold values from -0.75 to 0.75
- readout_imaginary: float32 [64, 16, 32], P('sp'), may hold values from -0.75 to 0.75
- skip_gain: float32 [64, 16], P('sp'), may hold values from -4 to 4
Outputs:
- grad_tokens: bfloat16 [8192, 2048], P('sp', 'dp')
- grad_in_weight: float32 [1024, 2048], P('sp', 'dp')
- grad_out_weight: float32 [1024, 2048], P('sp', 'dp')
The draws below stay inside these ranges and needn't reach their ends.
All inputs are finite; a program needn't handle non-finite values.
Results may differ from the reference program's by a relative error of at most 0.02.
Values may be sent and summed in bfloat16 or wider, within the bound.
A program may use at most 64 MiB of HBM per device.

```python
import math
import jax
import jax.numpy as jnp
from jax import lax

D = 2048
C = 16
P_SIZE = 32
GROUPS = 64
DSSM = 1024
LENGTH = 8192
N_DP = 8


def draw_decay_rate(key, part):
    own_key = jax.random.fold_in(key, 5)
    pick_key, slow_key, fast_key = jax.random.split(own_key, 3)
    slow_share = 0.5
    chooser = jax.random.uniform(pick_key, (GROUPS, P_SIZE), jnp.float32)
    slow_value = jax.random.uniform(slow_key, (GROUPS, P_SIZE), jnp.float32, math.log(0.07), math.log(0.1))
    fast_value = jax.random.uniform(fast_key, (GROUPS, P_SIZE), jnp.float32, math.log(0.3), math.log(0.6))
    return jnp.exp(jnp.where(chooser < slow_share, slow_value, fast_value)).astype(jnp.float32)


def position_envelope(key):
    block_count = (LENGTH + 15) // 16
    loud = jax.random.uniform(key, (block_count,), jnp.float32) < 0.25
    levels = jnp.where(loud, 1.0, 0.15).astype(jnp.float32)
    return jnp.repeat(levels, 16)[:LENGTH]


def enveloped_rows(key):
    level_key, value_key = jax.random.split(key)
    values = jax.random.truncated_normal(value_key, -6.0, 6.0, (LENGTH, D), jnp.float32)
    return (values * position_envelope(level_key)[:, None]).astype(jnp.bfloat16)


def draw_tokens(key, part):
    return enveloped_rows(jax.random.fold_in(key, 11))


def draw_cotangent(key, part):
    return enveloped_rows(jax.random.fold_in(key, 23))


def steps_of(stream_key, dims, cuts, least, largest):
    factor_of = 1.0
    for axis_at, shards_of in cuts:
        draws = jax.random.uniform(jax.random.fold_in(jax.random.fold_in(stream_key, 6), axis_at), (shards_of,), jnp.float32, least / len(cuts), largest / len(cuts))
        factor_of = factor_of * jnp.repeat(jnp.exp(draws), dims[axis_at] // shards_of).reshape((-1,) + (1,) * (len(dims) - 1 - axis_at))
    return factor_of


def normal_values(rng, dims, scale, limit, cuts=(), held_as=jnp.bfloat16):
    loudness = steps_of(rng, dims, cuts, -0.22, 0.18) if cuts else 1.0
    result = jax.random.normal(rng, dims, jnp.float32) * scale * loudness
    return jnp.minimum(jnp.maximum(result, -limit), limit).astype(held_as)


def setup_inputs(seed: int = 0) -> dict:
    keys = jax.random.split(jax.random.key(seed), 13)
    return {
        "tokens": draw_tokens(jax.random.fold_in(keys[12], 71), 0),
        "cotangent": draw_cotangent(jax.random.fold_in(keys[12], 71), 0),
        "in_weight": normal_values(keys[2], (DSSM, D), D ** -0.5, 0.125, ((0, 64), (1, 8))),
        "out_weight": normal_values(keys[3], (DSSM, D), DSSM ** -0.5, 0.1875, ((0, 64), (1, 8))),
        "decay_rate": draw_decay_rate(jax.random.fold_in(keys[12], 71), 0),
        "frequency": jnp.clip(4.0 + 36.0 * jax.random.uniform(keys[5], (GROUPS, P_SIZE), jnp.float32) ** steps_of(keys[5], (GROUPS, P_SIZE), ((0, 64),), -0.2, 0.2), 4.0, 40.0),
        "step_log": jnp.clip(-2.6593 + 0.6932001 * jax.random.uniform(keys[6], (GROUPS,), jnp.float32) ** steps_of(keys[6], (GROUPS,), ((0, 64),), -0.2, 0.2), -2.6593, -1.9661),
        "drive_real": normal_values(keys[7], (GROUPS, P_SIZE, C), 0.6, 6.0, ((0, 64),), jnp.float32),
        "drive_imag": normal_values(keys[8], (GROUPS, P_SIZE, C), 0.6, 6.0, ((0, 64),), jnp.float32),
        "readout_real_part": normal_values(keys[9], (GROUPS, C, P_SIZE), (2 * P_SIZE) ** -0.5, 0.75, ((0, 64),), jnp.float32),
        "readout_imaginary": normal_values(keys[10], (GROUPS, C, P_SIZE), (2 * P_SIZE) ** -0.5, 0.75, ((0, 64),), jnp.float32),
        "skip_gain": normal_values(keys[11], (GROUPS, C), 0.3, 4.0, ((0, 64),), jnp.float32),
    }


finest_precision = lax.Precision.HIGHEST

def combine(earlier, later):
    first_real, first_imag, first_sum_real, first_sum_imag = earlier
    next_real, next_imag, next_sum_real, next_sum_imag = later
    return (first_real * next_real - first_imag * next_imag, first_real * next_imag + first_imag * next_real, next_real * first_sum_real - next_imag * first_sum_imag + next_sum_real, next_real * first_sum_imag + next_imag * first_sum_real + next_sum_imag)

def discretize(decay_rate, frequency, step_log, drive_real, drive_imag):
    step_size = jnp.exp(step_log)[..., None]
    magnitude = jnp.exp(-decay_rate * step_size)
    angle = frequency * step_size
    decay_real = magnitude * jnp.cos(angle)
    decay_imag = magnitude * jnp.sin(angle)
    modulus = decay_rate * decay_rate + frequency * frequency
    hold_real = (-decay_rate * (decay_real - 1.0) + frequency * decay_imag) / modulus
    hold_imag = (-frequency * (decay_real - 1.0) - decay_rate * decay_imag) / modulus
    input_real = hold_real[..., None] * drive_real - hold_imag[..., None] * drive_imag
    input_imag = hold_real[..., None] * drive_imag + hold_imag[..., None] * drive_real
    return (decay_real, decay_imag, input_real, input_imag)

def one_group(inputs):
    drive_rows, back_rows, decay_rate, frequency, step_log, drive_real, drive_imag, readout_real_part, readout_imaginary, skip_gain = inputs
    decay_real, decay_imag, input_real, input_imag = discretize(decay_rate, frequency, step_log, drive_real, drive_imag)
    length = drive_rows.shape[1]
    factor_real = jnp.broadcast_to(decay_real[:, None], (decay_real.shape[0], length))
    factor_imag = jnp.broadcast_to(decay_imag[:, None], (decay_imag.shape[0], length))
    push_real = jnp.einsum('pc,ck->pk', input_real, drive_rows, precision=finest_precision)
    push_imag = jnp.einsum('pc,ck->pk', input_imag, drive_rows, precision=finest_precision)
    _, _, state_real, state_imag = lax.associative_scan(combine, (factor_real, factor_imag, push_real, push_imag), axis=1)
    mixed_rows = jnp.einsum('cp,pk->ck', readout_real_part, state_real, precision=finest_precision) - jnp.einsum('cp,pk->ck', readout_imaginary, state_imag, precision=finest_precision) + skip_gain[:, None] * drive_rows
    gated, pullback = jax.vjp(jax.nn.gelu, mixed_rows)
    interior_gradient, = pullback(back_rows)
    pulled_real_part = jnp.einsum('cp,ck->pk', readout_real_part, interior_gradient, precision=finest_precision)[:, ::-1]
    pulled_imaginary = -jnp.einsum('cp,ck->pk', readout_imaginary, interior_gradient, precision=finest_precision)[:, ::-1]
    _, _, adjoint_real, adjoint_imag = lax.associative_scan(combine, (factor_real, -factor_imag, pulled_real_part, pulled_imaginary), axis=1)
    adjoint_real = adjoint_real[:, ::-1]
    adjoint_imag = adjoint_imag[:, ::-1]
    grad_rows = jnp.einsum('pc,pk->ck', input_real, adjoint_real, precision=finest_precision) + jnp.einsum('pc,pk->ck', input_imag, adjoint_imag, precision=finest_precision) + skip_gain[:, None] * interior_gradient
    return (grad_rows.astype(jnp.bfloat16), gated.astype(jnp.bfloat16))

def reference(tokens, cotangent, in_weight, out_weight, decay_rate, frequency, step_log, drive_real, drive_imag, readout_real_part, readout_imaginary, skip_gain):
    block_width = D // N_DP
    drive_sum = jnp.zeros((DSSM, LENGTH), jnp.float32)
    back_sum = jnp.zeros((DSSM, LENGTH), jnp.float32)
    for column_block in range(N_DP):
        low = column_block * block_width
        token_cols = tokens[:, low:low + block_width]
        cot_cols = cotangent[:, low:low + block_width]
        part_drive = jnp.dot(in_weight[:, low:low + block_width], token_cols.T, preferred_element_type=jnp.float32)
        part_back = jnp.dot(out_weight[:, low:low + block_width], cot_cols.T, preferred_element_type=jnp.float32)
        drive_sum = drive_sum + lax.optimization_barrier(part_drive.astype(jnp.bfloat16)).astype(jnp.float32)
        back_sum = back_sum + lax.optimization_barrier(part_back.astype(jnp.bfloat16)).astype(jnp.float32)
    projected = drive_sum.astype(jnp.bfloat16)
    back_mix = back_sum.astype(jnp.bfloat16)
    drive_groups = projected.astype(jnp.float32).reshape(GROUPS, C, LENGTH)
    back_groups = back_mix.astype(jnp.float32).reshape(GROUPS, C, LENGTH)
    grad_groups, gated_groups = lax.map(one_group, (drive_groups, back_groups, decay_rate, frequency, step_log, drive_real, drive_imag, readout_real_part, readout_imaginary, skip_gain))
    grad_mix = grad_groups.reshape(DSSM, LENGTH)
    gated = gated_groups.reshape(DSSM, LENGTH)
    grad_tokens = jnp.dot(grad_mix.T, in_weight, preferred_element_type=jnp.float32).astype(jnp.bfloat16)
    grad_scale = LENGTH ** (-0.5)
    grad_in_weight = jnp.dot(grad_mix, tokens, preferred_element_type=jnp.float32) * grad_scale
    grad_out_weight = jnp.dot(gated, cotangent, preferred_element_type=jnp.float32) * grad_scale
    return (grad_tokens, grad_in_weight, grad_out_weight)
```

```python
import functools
import math

import jax
import jax.numpy as jnp
from jax import lax
from jax.experimental import pallas as pl
from jax.experimental.pallas import tpu as pltpu
from jax.sharding import PartitionSpec as P

MESH = pl.DeviceIdType.MESH
F32 = jnp.float32
BF16 = jnp.bfloat16
HIGHEST = lax.Precision.HIGHEST

(
    IN_A1, IN_B1, IN_A2, IN_B2, OUT_A1, OUT_B1, OUT_A2, OUT_B2,
    PK_Z, AUX_Z, PK_Y, AUX_Y, DRIVE, BACK, FWD_Y, FWD_Z, BWD_Y, BWD_Z,
    GATED, MIX, GO_A1, GO_B1, GO_A2, GO_B2, GI_A1, GI_B1, GI_A2, GI_B2,
) = range(28)
PHASES = 28

NN = (((1,), (0,)), ((), ()))
NT = (((1,), (1,)), ((), ()))
TN = (((0,), (0,)), ((), ()))


def dot(a, b, dims=NN, precision=None):
    return lax.dot_general(a, b, dims, precision=precision, preferred_element_type=F32)


def cmul(a, b):
    return a[0] * b[0] - a[1] * b[1], a[0] * b[1] + a[1] * b[0]


def conj(a):
    return a[0], -a[1]


def square(a, times):
    for _ in range(times):
        a = (a[0] * a[0] - a[1] * a[1], 2.0 * a[0] * a[1])
    return a


def log2(n):
    return n.bit_length() - 1


def iota(shape, dim):
    return lax.broadcasted_iota(jnp.int32, shape, dim)


def scan_rows(pair, decay, reverse):
    re, im = pair
    rows, lanes = re.shape
    width = min(128, lanes)
    row = iota((rows, width), 0)
    outs = []
    for at in range(0, lanes, width):
        a, b = re[:, at : at + width], im[:, at : at + width]
        f = (decay[0][:, at : at + width], decay[1][:, at : at + width])
        for k in range(log2(rows)):
            step = 1 << k
            if reverse:
                turn, keep = rows - step, row < rows - step
            else:
                turn, keep = step, row >= step
            ra = jnp.where(keep, pltpu.roll(a, turn, 0), 0.0)
            rb = jnp.where(keep, pltpu.roll(b, turn, 0), 0.0)
            a, b = a + f[0] * ra - f[1] * rb, b + f[0] * rb + f[1] * ra
            f = square(f, 1)
        outs.append((a, b))
    return (
        jnp.concatenate([o[0] for o in outs], axis=1),
        jnp.concatenate([o[1] for o in outs], axis=1),
    )


def kernel(
    ny, nz, nd,
    tok, cot, win, wout, rate, freq, slog, dr, di, rr, ri, skip,
    o_tok, o_in, o_out,
    pk_own, aux_own, pk_z, aux_z, pk_y, aux_y,
    wa_in, wb_in, wa_out, wb_out,
    d_send, d_recv, b_send, b_recv,
    f_own, f_recv, t_own, t_recv, a_own, a_recv, q_own, q_recv,
    gat_own, gat_all, mix_own, mix_all,
    go_sa, go_sb, go_ra, go_rb, go_s2a, go_s2b, go_r2a, go_r2b,
    gi_sa, gi_sb, gi_ra, gi_rb, gi_s2a, gi_s2b, gi_r2a, gi_r2b,
    bre, bim, cre, cim, u_re, u_im, v_re, v_im,
    ssem, rsem,
):
    sp, dp = lax.axis_index("sp"), lax.axis_index("dp")
    z, y = lax.div(sp, ny), lax.rem(sp, ny)
    size = {"y": ny, "z": nz, "d": nd}
    here = {"y": y, "z": z, "d": dp}
    rows = tok.shape[0]
    states = rate.shape[1]
    per_group = skip.shape[1]
    own_ch = ny * per_group
    lanes = ny * states
    half = win.shape[1] // 2

    def device(axis, j):
        if axis == "y":
            return (z * ny + j, dp)
        if axis == "z":
            return (j * ny + y, dp)
        return (sp, j)

    def copy(phase, axis, k, src, dst):
        j = lax.rem(here[axis] + k, size[axis])
        return pltpu.make_async_remote_copy(
            src_ref=src(j),
            dst_ref=dst,
            send_sem=ssem.at[phase, k],
            recv_sem=rsem.at[phase, k],
            device_id=device(axis, j),
            device_id_type=MESH,
        )

    sent = []

    def send(phase, axis, src, dst):
        for k in range(1, size[axis]):
            copy(phase, axis, k, src, dst).start()
        sent.append((phase, axis, src, dst))

    def arrive(phase, axis, slot):
        n = size[axis]
        for k in range(1, n):
            j = lax.rem(here[axis] + (n - k), n)
            copy(phase, axis, k, lambda _: slot(j), slot(j)).wait_recv()

    barrier = pltpu.get_barrier_semaphore()
    for axis in ("y", "z", "d"):
        for k in range(1, size[axis]):
            j = lax.rem(here[axis] + k, size[axis])
            pl.semaphore_signal(barrier, inc=1, device_id=device(axis, j), device_id_type=MESH)

    tile_s = (iota((states, lanes), 0) == lax.rem(iota((states, lanes), 1), states)).astype(F32)
    wide = lambda ref: dot(jnp.broadcast_to(ref[...], (8, states)), tile_s, precision=HIGHEST)
    rate_w, freq_w = wide(rate), wide(freq)
    step = jnp.exp(jnp.full((8, lanes), slog[0], F32))
    magnitude = jnp.exp(-rate_w * step)
    angle = freq_w * step
    dec_re, dec_im = magnitude * jnp.cos(angle), magnitude * jnp.sin(angle)
    modulus = rate_w * rate_w + freq_w * freq_w
    hold_re = (-rate_w * (dec_re - 1.0) + freq_w * dec_im) / modulus
    hold_im = (-freq_w * (dec_re - 1.0) - rate_w * dec_im) / modulus
    tile_c = (
        iota((per_group, lanes), 0) == lax.rem(iota((per_group, lanes), 1), per_group)
    ).astype(F32)
    skip_w = dot(jnp.broadcast_to(skip[...], (8, per_group)), tile_c, precision=HIGHEST)
    row8 = iota((8, lanes), 0)
    aux_own[...] = jnp.where(row8 == 0, dec_re, jnp.where(row8 == 1, dec_im, skip_w))
    four = 4 * states
    p_row, p_lane = iota((states, four), 0), iota((states, four), 1)
    hr, hi = hold_re[0:1, 0:states], hold_im[0:1, 0:states]
    hr = jnp.concatenate([hr] * 4, axis=1) if four > lanes else hold_re[0:1, 0:four]
    hi = jnp.concatenate([hi] * 4, axis=1) if four > lanes else hold_im[0:1, 0:four]
    first, second = p_lane == p_row, p_lane == p_row + states
    sel_r = jnp.where(first, hr, 0.0) + jnp.where(second, hi, 0.0)
    sel_i = jnp.where(first, -hi, 0.0) + jnp.where(second, hr, 0.0)
    sel_c = (p_lane == p_row + 2 * states).astype(F32)
    sel_d = (p_lane == p_row + 3 * states).astype(F32)
    pk_own[...] = (
        dot(dr[0], sel_r, NN, HIGHEST)
        + dot(di[0], sel_i, NN, HIGHEST)
        + dot(rr[0], sel_c, NN, HIGHEST)
        + dot(ri[0], sel_d, NN, HIGHEST)
    ).astype(BF16)

    pl.semaphore_wait(barrier, (ny - 1) + (nz - 1) + (nd - 1))

    send(IN_A1, "y", lambda j: win.at[:, 0:half], wa_in.at[z, y])
    send(IN_B1, "z", lambda j: win.at[:, half:], wb_in.at[y, z])

    def param_copy(phase, k, src, dst):
        j = lax.rem(z + k, nz)
        return pltpu.make_async_remote_copy(
            src_ref=src, dst_ref=dst, send_sem=ssem.at[phase, k], recv_sem=rsem.at[phase, 0],
            device_id=(j * ny + y, dp), device_id_type=MESH,
        )

    @pl.when(z == dp)
    def _():
        for k in range(1, nz):
            param_copy(PK_Z, k, pk_own, pk_z).start()
            param_copy(AUX_Z, k, aux_own, aux_z).start()
        pk_z[...] = pk_own[...]
        aux_z[...] = aux_own[...]

    send(OUT_A1, "y", lambda j: wout.at[:, 0:half], wa_out.at[z, y])
    send(OUT_B1, "z", lambda j: wout.at[:, half:], wb_out.at[y, z])
    wa_in[z, y] = win[:, 0:half]
    wb_in[y, z] = win[:, half:]
    wa_out[z, y] = wout[:, 0:half]
    wb_out[y, z] = wout[:, half:]

    arrive(IN_A1, "y", lambda j: wa_in.at[z, j])
    send(IN_A2, "z", lambda j: wa_in.at[z], wa_in.at[z])
    arrive(IN_B1, "z", lambda j: wb_in.at[y, j])
    send(IN_B2, "y", lambda j: wb_in.at[y], wb_in.at[y])

    @pl.when(z != dp)
    def _():
        param_copy(PK_Z, 1, pk_z, pk_z).wait_recv()
        param_copy(AUX_Z, 1, aux_z, aux_z).wait_recv()

    send(PK_Y, "y", lambda j: pk_z, pk_y.at[y])
    send(AUX_Y, "y", lambda j: aux_z, aux_y.at[y])
    pk_y[y] = pk_z[...]
    aux_y[y] = aux_z[...]

    arrive(OUT_A1, "y", lambda j: wa_out.at[z, j])
    send(OUT_A2, "z", lambda j: wa_out.at[z], wa_out.at[z])
    arrive(OUT_B1, "z", lambda j: wb_out.at[y, j])
    send(OUT_B2, "y", lambda j: wb_out.at[y], wb_out.at[y])

    arrive(PK_Y, "y", lambda j: pk_y.at[j])
    arrive(AUX_Y, "y", lambda j: aux_y.at[j])
    packed = pk_y[...].reshape(own_ch, four)
    diag = lax.div(iota((own_ch, lanes), 0), per_group) == lax.div(iota((own_ch, lanes), 1), states)
    s_row, s_lane = iota((four, lanes), 0), lax.rem(iota((four, lanes), 1), states)
    for at, ref in enumerate((bre, bim, cre, cim)):
        spread = (s_row == s_lane + at * states).astype(F32).astype(BF16)
        ref[...] = jnp.where(diag, dot(packed, spread), 0.0).astype(BF16)
    group_of_lane = lax.div(iota((1, lanes), 1), states)
    group_of_ch = lax.div(iota((1, own_ch), 1), per_group)
    dec = (jnp.zeros((1, lanes), F32), jnp.zeros((1, lanes), F32))
    gain = jnp.zeros((1, own_ch), F32)
    for g in range(ny):
        dec = (
            jnp.where(group_of_lane == g, aux_y[g, 0:1, :], dec[0]),
            jnp.where(group_of_lane == g, aux_y[g, 1:2, :], dec[1]),
        )
        gain = jnp.where(group_of_ch == g, aux_y[g, 2:3, 0:own_ch], gain)
    row = iota((rows, lanes), 0)
    up = (jnp.ones((rows, lanes), F32), jnp.zeros((rows, lanes), F32))
    down = up
    factor = dec
    for k in range(log2(rows)):
        bit = lax.rem(lax.div(row, 1 << k), 2) == 1
        more = cmul(up, factor)
        up = (jnp.where(bit, more[0], up[0]), jnp.where(bit, more[1], up[1]))
        more = cmul(down, factor)
        down = (jnp.where(bit, down[0], more[0]), jnp.where(bit, down[1], more[1]))
        factor = square(factor, 1)
    u_re[...], u_im[...] = up
    v_re[...], v_im[...] = down
    dec_chunk = factor
    dec_row = square(dec_chunk, log2(ny))

    def weights_of(wa, wb, b):
        left = wa[b].reshape(own_ch, half)
        right = wb[:, b].reshape(own_ch, half)
        return jnp.concatenate([left, right], axis=1)

    def gathered(phase_a, phase_b, wa, wb):
        arrive(phase_a, "z", lambda j: wa.at[j])
        arrive(phase_b, "y", lambda j: wb.at[j])

    def project(act, wa, wb, out):
        for b in range(nd):
            out[b] = dot(act[...], weights_of(wa, wb, b), NT).astype(BF16)

    def total(recv):
        s = recv[0].astype(F32)
        for b in range(1, nd):
            s = s + recv[b].astype(F32)
        return s.astype(BF16)

    gathered(IN_A2, IN_B2, wa_in, wb_in)
    project(tok, wa_in, wb_in, d_send)
    send(DRIVE, "d", lambda j: d_send.at[j], d_recv.at[dp])
    d_recv[dp] = d_send[dp]
    arrive(DRIVE, "d", lambda j: d_recv.at[j])
    x = total(d_recv)

    def carried(recv, n, me, decay, reverse):
        zero = jnp.zeros((1, lanes), F32)
        enter, whole, power = (zero, zero), (zero, zero), (zero + 1.0, zero)
        for i in range(n):
            j = n - 1 - i if reverse else i
            piece = (recv[j, 0:1, :], recv[j, 1:2, :])
            before = j > me if reverse else j < me
            grown = cmul(enter, decay)
            enter = (
                jnp.where(before, grown[0] + piece[0], enter[0]),
                jnp.where(before, grown[1] + piece[1], enter[1]),
            )
            grown = cmul(whole, decay)
            whole = (grown[0] + piece[0], grown[1] + piece[1])
            grown = cmul(power, decay)
            power = (
                jnp.where(before, grown[0], power[0]),
                jnp.where(before, grown[1], power[1]),
            )
        return enter, whole, power

    def summed(pair, table_re, table_im, sign):
        tr, ti = table_re[...], sign * table_im[...]
        re, im = cmul(pair, (tr, ti))
        return jnp.sum(re, axis=0, keepdims=True), jnp.sum(im, axis=0, keepdims=True)

    def put(ref, pair):
        ref[0:1, :] = pair[0]
        ref[1:2, :] = pair[1]

    push = (dot(x, bre[...]), dot(x, bim[...]))
    final = summed(push, v_re, v_im, 1.0)
    put(f_own, final)
    send(FWD_Y, "y", lambda j: f_own, f_recv.at[y])
    put(f_recv.at[y], final)
    local = scan_rows(push, dec, False)
    arrive(FWD_Y, "y", lambda j: f_recv.at[j])
    enter_y, whole_y, power_y = carried(f_recv, ny, y, dec_chunk, False)
    put(t_own, whole_y)
    send(FWD_Z, "z", lambda j: t_own, t_recv.at[z])
    put(t_recv.at[z], whole_y)

    gathered(OUT_A2, OUT_B2, wa_out, wb_out)
    project(cot, wa_out, wb_out, b_send)
    send(BACK, "d", lambda j: b_send.at[j], b_recv.at[dp])
    b_recv[dp] = b_send[dp]

    arrive(FWD_Z, "z", lambda j: t_recv.at[j])
    enter_z, _, _ = carried(t_recv, nz, z, dec_row, False)
    far = cmul(power_y, enter_z)
    start = cmul(dec, (enter_y[0] + far[0], enter_y[1] + far[1]))
    add = cmul((u_re[...], u_im[...]), start)
    state_re, state_im = (local[0] + add[0]).astype(BF16), (local[1] + add[1]).astype(BF16)
    mixed = dot(state_re, cre[...], NT) - dot(state_im, cim[...], NT) + gain * x.astype(F32)
    c0 = math.sqrt(2.0 / math.pi)
    sq = mixed * mixed
    th = jnp.tanh(c0 * mixed * (1.0 + 0.044715 * sq))
    half_up = 0.5 * (1.0 + th)
    gated = (mixed * half_up).astype(BF16)
    slope = half_up + 0.5 * mixed * (1.0 - th * th) * (c0 * (1.0 + 3.0 * 0.044715 * sq))
    gat_own[...] = gated
    send(GATED, "d", lambda j: gat_own, gat_all.at[dp])
    gat_all[dp] = gated

    arrive(BACK, "d", lambda j: b_recv.at[j])
    inner = slope * total(b_recv).astype(F32)
    inner_b = inner.astype(BF16)
    pulled = (dot(inner_b, cre[...]), -dot(inner_b, cim[...]))
    opening = summed(pulled, u_re, u_im, -1.0)
    put(a_own, opening)
    send(BWD_Y, "y", lambda j: a_own, a_recv.at[y])
    put(a_recv.at[y], opening)
    back_dec = conj(dec)
    local = scan_rows(pulled, back_dec, True)
    arrive(BWD_Y, "y", lambda j: a_recv.at[j])
    enter_y, whole_y, power_y = carried(a_recv, ny, y, conj(dec_chunk), True)
    put(q_own, whole_y)
    send(BWD_Z, "z", lambda j: q_own, q_recv.at[z])
    put(q_recv.at[z], whole_y)

    def weight_grad(phase_a, phase_b, cols, act, sa, sb, ra, rb):
        for b in range(nd):
            part = dot(cols[b], act[...], TN).astype(BF16)
            sa[b] = part[:, 0:half].reshape(ny, per_group, half)
            sb[:, b] = part[:, half:].reshape(ny, per_group, half)
        send(phase_a, "z", lambda j: sa.at[j], ra.at[z])
        send(phase_b, "y", lambda j: sb.at[j], rb.at[y])
        ra[z] = sa[z]
        rb[y] = sb[y]

    def reduced(recv, n):
        s = recv[0].astype(F32)
        for j in range(1, n):
            s = s + recv[j].astype(F32)
        return s

    def second_step(phase_a1, phase_b1, phase_a2, phase_b2, ra, rb, s2a, s2b, r2a, r2b):
        arrive(phase_a1, "z", lambda j: ra.at[j])
        s2a[...] = reduced(ra, nz).astype(BF16)
        send(phase_a2, "y", lambda j: s2a.at[j], r2a.at[y])
        r2a[y] = s2a[y]
        arrive(phase_b1, "y", lambda j: rb.at[j])
        s2b[...] = reduced(rb, ny).astype(BF16)
        send(phase_b2, "z", lambda j: s2b.at[j], r2b.at[z])
        r2b[z] = s2b[z]

    scale = (rows * ny * nz) ** -0.5

    def finish(phase_a2, phase_b2, r2a, r2b, out):
        arrive(phase_a2, "y", lambda j: r2a.at[j])
        arrive(phase_b2, "z", lambda j: r2b.at[j])
        out[:, 0:half] = reduced(r2a, ny) * scale
        out[:, half:] = reduced(r2b, nz) * scale

    arrive(GATED, "d", lambda j: gat_all.at[j])
    weight_grad(GO_A1, GO_B1, gat_all, cot, go_sa, go_sb, go_ra, go_rb)

    arrive(BWD_Z, "z", lambda j: q_recv.at[j])
    enter_z, _, _ = carried(q_recv, nz, z, conj(dec_row), True)
    far = cmul(power_y, enter_z)
    start = cmul(back_dec, (enter_y[0] + far[0], enter_y[1] + far[1]))
    add = cmul((v_re[...], -v_im[...]), start)
    adj_re, adj_im = (local[0] + add[0]).astype(BF16), (local[1] + add[1]).astype(BF16)
    mix = (dot(adj_re, bre[...], NT) + dot(adj_im, bim[...], NT) + gain * inner).astype(BF16)
    mix_own[...] = mix
    send(MIX, "d", lambda j: mix_own, mix_all.at[dp])
    mix_all[dp] = mix

    second_step(GO_A1, GO_B1, GO_A2, GO_B2, go_ra, go_rb, go_s2a, go_s2b, go_r2a, go_r2b)
    arrive(MIX, "d", lambda j: mix_all.at[j])
    weight_grad(GI_A1, GI_B1, mix_all, tok, gi_sa, gi_sb, gi_ra, gi_rb)
    grad = dot(mix_all[0], weights_of(wa_in, wb_in, 0))
    for b in range(1, nd):
        grad = grad + dot(mix_all[b], weights_of(wa_in, wb_in, b))
    o_tok[...] = grad.astype(BF16)
    finish(GO_A2, GO_B2, go_r2a, go_r2b, o_out)
    second_step(GI_A1, GI_B1, GI_A2, GI_B2, gi_ra, gi_rb, gi_s2a, gi_s2b, gi_r2a, gi_r2b)
    finish(GI_A2, GI_B2, gi_r2a, gi_r2b, o_in)

    @pl.when(z == dp)
    def _():
        for k in range(1, nz):
            param_copy(PK_Z, k, pk_own, pk_z).wait_send()
            param_copy(AUX_Z, k, aux_own, aux_z).wait_send()

    for phase, axis, src, dst in sent:
        for k in range(1, size[axis]):
            copy(phase, axis, k, src, dst).wait_send()


def on_device(ny, nz, nd, tok, cot, win, wout, rate, freq, slog, dr, di, rr, ri, skip):
    rows, cols = tok.shape
    half = cols // 2
    states, c = rate.shape[1], skip.shape[1]
    own_ch, lanes, four = ny * c, ny * states, 4 * states
    V = pltpu.VMEM
    grads = [
        V((nz, ny, c, half), BF16), V((ny, nz, c, half), BF16),
        V((nz, ny, c, half), BF16), V((ny, nz, c, half), BF16),
        V((ny, c, half), BF16), V((nz, c, half), BF16),
        V((ny, c, half), BF16), V((nz, c, half), BF16),
    ]
    most = max(ny, nz, nd)
    vm = pl.BlockSpec(memory_space=pltpu.VMEM)
    return pl.pallas_call(
        functools.partial(kernel, ny, nz, nd),
        out_shape=(
            jax.ShapeDtypeStruct((rows, cols), BF16),
            jax.ShapeDtypeStruct(win.shape, F32),
            jax.ShapeDtypeStruct(wout.shape, F32),
        ),
        in_specs=[vm] * 6 + [pl.BlockSpec(memory_space=pltpu.SMEM)] + [vm] * 5,
        out_specs=(vm, vm, vm),
        scratch_shapes=[
            V((c, four), BF16), V((8, lanes), F32),
            V((c, four), BF16), V((8, lanes), F32),
            V((ny, c, four), BF16), V((ny, 8, lanes), F32),
            V((nz, ny, c, half), BF16), V((ny, nz, c, half), BF16),
            V((nz, ny, c, half), BF16), V((ny, nz, c, half), BF16),
            V((nd, rows, own_ch), BF16), V((nd, rows, own_ch), BF16),
            V((nd, rows, own_ch), BF16), V((nd, rows, own_ch), BF16),
            V((2, lanes), F32), V((ny, 2, lanes), F32),
            V((2, lanes), F32), V((nz, 2, lanes), F32),
            V((2, lanes), F32), V((ny, 2, lanes), F32),
            V((2, lanes), F32), V((nz, 2, lanes), F32),
            V((rows, own_ch), BF16), V((nd, rows, own_ch), BF16),
            V((rows, own_ch), BF16), V((nd, rows, own_ch), BF16),
            *grads, *grads,
            *[V((own_ch, lanes), BF16)] * 4,
            *[V((rows, lanes), F32)] * 4,
            pltpu.SemaphoreType.DMA((PHASES, most)),
            pltpu.SemaphoreType.DMA((PHASES, most)),
        ],
        compiler_params=pltpu.CompilerParams(
            collective_id=0, has_side_effects=True, vmem_limit_bytes=48 * 1024 * 1024
        ),
        name="mixer",
    )(tok, cot, win, wout, rate, freq, slog, jnp.swapaxes(dr, 1, 2), jnp.swapaxes(di, 1, 2), rr, ri, skip)


def solution(mesh):
    nd = mesh.shape["dp"]
    nz = nd
    ny = mesh.shape["sp"] // nz
    return jax.shard_map(
        functools.partial(on_device, ny, nz, nd),
        mesh=mesh,
        in_specs=(
            P("sp", "dp"), P("sp", "dp"), P("sp", "dp"), P("sp", "dp"),
            P("sp", None), P("sp", None), P("sp"),
            P("sp", None, None), P("sp", None, None), P("sp", None, None), P("sp", None, None),
            P("sp", None),
        ),
        out_specs=(P("sp", "dp"), P("sp", "dp"), P("sp", "dp")),
        check_vma=False,
    )
```

```python
import functools
import math

import jax
import jax.numpy as jnp
from jax import lax
from jax.experimental import pallas as pl
from jax.experimental.pallas import tpu as pltpu
from jax.sharding import PartitionSpec as P

MESH = pl.DeviceIdType.MESH
F32 = jnp.float32
BF16 = jnp.bfloat16
HIGHEST = lax.Precision.HIGHEST

(
    IN_A1, IN_B1, IN_A2, IN_B2, OUT_A1, OUT_B1, OUT_A2, OUT_B2,
    PK_Z, AUX_Z, PK_Y, AUX_Y, DRIVE, BACK, FWD_Y, FWD_Z, BWD_Y, BWD_Z,
    GATED, MIX, GO_A1, GO_B1, GO_A2, GO_B2, GI_A1, GI_B1, GI_A2, GI_B2,
) = range(28)
PHASES = 28

NN = (((1,), (0,)), ((), ()))
NT = (((1,), (1,)), ((), ()))
TN = (((0,), (0,)), ((), ()))


def dot(a, b, dims=NN, precision=None):
    return lax.dot_general(a, b, dims, precision=precision, preferred_element_type=F32)


def cmul(a, b):
    return a[0] * b[0] - a[1] * b[1], a[0] * b[1] + a[1] * b[0]


def conj(a):
    return a[0], -a[1]


def square(a, times):
    for _ in range(times):
        a = (a[0] * a[0] - a[1] * a[1], 2.0 * a[0] * a[1])
    return a


def ring_order(n, far_first):
    ks = sorted(range(1, n), key=lambda k: (min(k, n - k), k))
    return ks[::-1] if far_first else ks


def log2(n):
    return n.bit_length() - 1


def iota(shape, dim):
    return lax.broadcasted_iota(jnp.int32, shape, dim)


def scan_rows(pair, decay, reverse):
    re, im = pair
    rows, lanes = re.shape
    width = min(128, lanes)
    row = iota((rows, width), 0)
    outs = []
    for at in range(0, lanes, width):
        a, b = re[:, at : at + width], im[:, at : at + width]
        f = (decay[0][:, at : at + width], decay[1][:, at : at + width])
        for k in range(log2(rows)):
            step = 1 << k
            if reverse:
                turn, keep = rows - step, row < rows - step
            else:
                turn, keep = step, row >= step
            ra = jnp.where(keep, pltpu.roll(a, turn, 0), 0.0)
            rb = jnp.where(keep, pltpu.roll(b, turn, 0), 0.0)
            a, b = a + f[0] * ra - f[1] * rb, b + f[0] * rb + f[1] * ra
            f = square(f, 1)
        outs.append((a, b))
    return (
        jnp.concatenate([o[0] for o in outs], axis=1),
        jnp.concatenate([o[1] for o in outs], axis=1),
    )


def kernel(
    ny, nz, nd,
    slog, tok_h, cot_h, win_h, wout_h, rate_h, freq_h, dr_h, di_h, rr_h, ri_h, skip_h,
    o_tok, o_in, o_out,
    tok, cot, win, wout, rate, freq, dr, di, rr, ri, skip,
    pk_own, aux_own, pk_z, aux_z, pk_y, aux_y,
    wa_in, wb_in, wa_out, wb_out,
    d_send, d_recv, b_send, b_recv,
    f_own, f_recv, t_own, t_recv, a_own, a_recv, q_own, q_recv,
    gat_own, gat_all, mix_own, mix_all,
    go_sa, go_sb, go_ra, go_rb, go_s2a, go_s2b, go_r2a, go_r2b,
    gi_sa, gi_sb, gi_ra, gi_rb, gi_s2a, gi_s2b, gi_r2a, gi_r2b,
    bre, bim, cre, cim, u_re, u_im, v_re, v_im,
    ssem, rsem, in1_sem, mix_sem, load_sem,
):
    sp, dp = lax.axis_index("sp"), lax.axis_index("dp")
    z, y = lax.div(sp, ny), lax.rem(sp, ny)
    size = {"y": ny, "z": nz, "d": nd}
    here = {"y": y, "z": z, "d": dp}
    rows = tok.shape[0]
    states = rate.shape[1]
    per_group = skip.shape[1]
    own_ch = ny * per_group
    lanes = ny * states
    half = win.shape[1] // 2

    def device(axis, j):
        if axis == "y":
            return (z * ny + j, dp)
        if axis == "z":
            return (j * ny + y, dp)
        return (sp, j)

    def peer(axis, k):
        return lax.rem(here[axis] + k, size[axis])

    def copy(phase, axis, j, src, dst, recv_sem=None):
        return pltpu.make_async_remote_copy(
            src_ref=src,
            dst_ref=dst,
            send_sem=ssem.at[phase],
            recv_sem=rsem.at[phase] if recv_sem is None else recv_sem,
            device_id=device(axis, j),
            device_id_type=MESH,
        )

    sent = []

    def send(phase, axis, src, dst, whole, sems=None):
        for k in ring_order(size[axis], True):
            j = peer(axis, k)
            copy(phase, axis, j, src(j), dst, None if sems is None else sems(k)).start()
        sent.append((phase, axis, whole))

    def arrive(phase, axis, whole):
        copy(phase, axis, peer(axis, 1), whole, whole).wait_recv()

    barrier = pltpu.get_barrier_semaphore()
    for axis in ("y", "z", "d"):
        for k in ring_order(size[axis], True):
            j = peer(axis, k)
            pl.semaphore_signal(barrier, inc=1, device_id=device(axis, j), device_id_type=MESH)

    pairs = (
        (rate_h, rate), (freq_h, freq), (dr_h, dr), (di_h, di), (rr_h, rr), (ri_h, ri),
        (skip_h, skip), (win_h, win), (wout_h, wout), (tok_h, tok), (cot_h, cot),
    )
    loads = [pltpu.make_async_copy(a, b, load_sem.at[i]) for i, (a, b) in enumerate(pairs)]
    for load in loads:
        load.start()
    for load in loads[:7]:
        load.wait()

    tile_s = (iota((states, lanes), 0) == lax.rem(iota((states, lanes), 1), states)).astype(F32)
    wide = lambda ref: dot(jnp.broadcast_to(ref[...], (8, states)), tile_s, precision=HIGHEST)
    rate_w, freq_w = wide(rate), wide(freq)
    step = jnp.exp(jnp.full((8, lanes), slog[0], F32))
    magnitude = jnp.exp(-rate_w * step)
    angle = freq_w * step
    dec_re, dec_im = magnitude * jnp.cos(angle), magnitude * jnp.sin(angle)
    modulus = rate_w * rate_w + freq_w * freq_w
    hold_re = (-rate_w * (dec_re - 1.0) + freq_w * dec_im) / modulus
    hold_im = (-freq_w * (dec_re - 1.0) - rate_w * dec_im) / modulus
    tile_c = (
        iota((per_group, lanes), 0) == lax.rem(iota((per_group, lanes), 1), per_group)
    ).astype(F32)
    skip_w = dot(jnp.broadcast_to(skip[...], (8, per_group)), tile_c, precision=HIGHEST)
    row8 = iota((8, lanes), 0)
    aux_own[...] = jnp.where(row8 == 0, dec_re, jnp.where(row8 == 1, dec_im, skip_w))
    four = 4 * states
    p_row, p_lane = iota((states, four), 0), iota((states, four), 1)
    hr, hi = hold_re[0:1, 0:states], hold_im[0:1, 0:states]
    hr = jnp.concatenate([hr] * 4, axis=1) if four > lanes else hold_re[0:1, 0:four]
    hi = jnp.concatenate([hi] * 4, axis=1) if four > lanes else hold_im[0:1, 0:four]
    first, second = p_lane == p_row, p_lane == p_row + states
    sel_r = jnp.where(first, hr, 0.0) + jnp.where(second, hi, 0.0)
    sel_i = jnp.where(first, -hi, 0.0) + jnp.where(second, hr, 0.0)
    sel_c = (p_lane == p_row + 2 * states).astype(F32)
    sel_d = (p_lane == p_row + 3 * states).astype(F32)
    pk_own[...] = (
        dot(dr[0], sel_r, NN, HIGHEST)
        + dot(di[0], sel_i, NN, HIGHEST)
        + dot(rr[0], sel_c, NN, HIGHEST)
        + dot(ri[0], sel_d, NN, HIGHEST)
    ).astype(BF16)

    pl.semaphore_wait(barrier, (ny - 1) + (nz - 1) + (nd - 1))

    def param_copy(phase, k, src, dst):
        return copy(phase, "z", peer("z", k), src, dst)

    @pl.when(z == dp)
    def _():
        for k in ring_order(nz, True):
            param_copy(PK_Z, k, pk_own, pk_z).start()
            param_copy(AUX_Z, k, aux_own, aux_z).start()
        pk_z[...] = pk_own[...]
        aux_z[...] = aux_own[...]

    for load in loads[7:9]:
        load.wait()
    near, far = ring_order(ny, False), ring_order(nz, False)

    def forward_a(j, src):
        for k in ring_order(nz, True):
            copy(IN_A2, "z", peer("z", k), src, wa_in.at[z, j]).start()

    def forward_b(j, src):
        for k in ring_order(ny, True):
            copy(IN_B2, "y", peer("y", k), src, wb_in.at[y, j]).start()

    left, right = win.at[:, 0:half], win.at[:, half:]
    send(IN_A1, "y", lambda j: left, wa_in.at[z, y], wa_in.at[0, 0 : ny - 1], lambda k: in1_sem.at[0, k])
    send(IN_B1, "z", lambda j: right, wb_in.at[y, z], wb_in.at[0, 0 : nz - 1], lambda k: in1_sem.at[1, k])
    forward_a(y, left)
    forward_b(z, right)
    wa_in[z, y] = win[:, 0:half]
    wb_in[y, z] = win[:, half:]
    wa_out[z, y] = wout[:, 0:half]
    wb_out[y, z] = wout[:, half:]
    for i in range(max(ny, nz) - 1):
        if i < ny - 1:
            k = near[i]
            j = peer("y", ny - k)
            copy(IN_A1, "y", j, left, wa_in.at[z, j], in1_sem.at[0, k]).wait_recv()
            forward_a(j, wa_in.at[z, j])
        if i < nz - 1:
            k = far[i]
            j = peer("z", nz - k)
            copy(IN_B1, "z", j, right, wb_in.at[y, j], in1_sem.at[1, k]).wait_recv()
            forward_b(j, wb_in.at[y, j])
        if i == 1 or max(ny, nz) == 2:
            send(OUT_A1, "y", lambda j: wout.at[:, 0:half], wa_out.at[z, y], wa_out.at[0, 0 : ny - 1])
            send(OUT_B1, "z", lambda j: wout.at[:, half:], wb_out.at[y, z], wb_out.at[0, 0 : nz - 1])
    sent.append((IN_A2, "z", wa_in.at[0 : nz - 1]))
    sent.append((IN_B2, "y", wb_in.at[0 : ny - 1]))

    @pl.when(z != dp)
    def _():
        param_copy(PK_Z, 1, pk_z, pk_z).wait_recv()
        param_copy(AUX_Z, 1, aux_z, aux_z).wait_recv()

    send(PK_Y, "y", lambda j: pk_z, pk_y.at[y], pk_y.at[0 : ny - 1])
    send(AUX_Y, "y", lambda j: aux_z, aux_y.at[y], aux_y.at[0 : ny - 1])
    pk_y[y] = pk_z[...]
    aux_y[y] = aux_z[...]

    arrive(OUT_A1, "y", wa_out.at[0, 0 : ny - 1])
    send(OUT_A2, "z", lambda j: wa_out.at[z], wa_out.at[z], wa_out.at[0 : nz - 1])
    arrive(OUT_B1, "z", wb_out.at[0, 0 : nz - 1])
    send(OUT_B2, "y", lambda j: wb_out.at[y], wb_out.at[y], wb_out.at[0 : ny - 1])

    def weights_of(wa, wb, b):
        left = wa[b].reshape(own_ch, half)
        right = wb[:, b].reshape(own_ch, half)
        return jnp.concatenate([left, right], axis=1)

    def gathered(phase_a, phase_b, wa, wb):
        arrive(phase_a, "z", wa.at[0 : nz - 1])
        arrive(phase_b, "y", wb.at[0 : ny - 1])

    def project(phase, act, wa, wb, out, recv):
        for k in ring_order(nd, True):
            j = peer("d", k)
            out[j] = dot(act[...], weights_of(wa, wb, j), NT).astype(BF16)
            copy(phase, "d", j, out.at[j], recv.at[dp]).start()
        sent.append((phase, "d", recv.at[0 : nd - 1]))
        recv[dp] = dot(act[...], weights_of(wa, wb, dp), NT).astype(BF16)

    for load in loads[9:]:
        load.wait()
    gathered(IN_A2, IN_B2, wa_in, wb_in)
    project(DRIVE, tok, wa_in, wb_in, d_send, d_recv)

    arrive(PK_Y, "y", pk_y.at[0 : ny - 1])
    arrive(AUX_Y, "y", aux_y.at[0 : ny - 1])
    packed = pk_y[...].reshape(own_ch, four)
    diag = lax.div(iota((own_ch, lanes), 0), per_group) == lax.div(iota((own_ch, lanes), 1), states)
    s_row, s_lane = iota((four, lanes), 0), lax.rem(iota((four, lanes), 1), states)
    for at, ref in enumerate((bre, bim, cre, cim)):
        spread = (s_row == s_lane + at * states).astype(F32).astype(BF16)
        ref[...] = jnp.where(diag, dot(packed, spread), 0.0).astype(BF16)
    group_of_lane = lax.div(iota((1, lanes), 1), states)
    group_of_ch = lax.div(iota((1, own_ch), 1), per_group)
    dec = (jnp.zeros((1, lanes), F32), jnp.zeros((1, lanes), F32))
    gain = jnp.zeros((1, own_ch), F32)
    for g in range(ny):
        dec = (
            jnp.where(group_of_lane == g, aux_y[g, 0:1, :], dec[0]),
            jnp.where(group_of_lane == g, aux_y[g, 1:2, :], dec[1]),
        )
        gain = jnp.where(group_of_ch == g, aux_y[g, 2:3, 0:own_ch], gain)
    row = iota((rows, lanes), 0)
    up = (jnp.ones((rows, lanes), F32), jnp.zeros((rows, lanes), F32))
    down = up
    factor = dec
    for k in range(log2(rows)):
        bit = lax.rem(lax.div(row, 1 << k), 2) == 1
        more = cmul(up, factor)
        up = (jnp.where(bit, more[0], up[0]), jnp.where(bit, more[1], up[1]))
        more = cmul(down, factor)
        down = (jnp.where(bit, down[0], more[0]), jnp.where(bit, down[1], more[1]))
        factor = square(factor, 1)
    u_re[...], u_im[...] = up
    v_re[...], v_im[...] = down
    dec_chunk = factor
    dec_row = square(dec_chunk, log2(ny))

    def total(recv):
        s = recv[0].astype(F32)
        for b in range(1, nd):
            s = s + recv[b].astype(F32)
        return s.astype(BF16)

    arrive(DRIVE, "d", d_recv.at[0 : nd - 1])
    x = total(d_recv)

    def carried(recv, n, me, decay, reverse):
        zero = jnp.zeros((1, lanes), F32)
        enter, whole, power = (zero, zero), (zero, zero), (zero + 1.0, zero)
        for i in range(n):
            j = n - 1 - i if reverse else i
            piece = (recv[j, 0:1, :], recv[j, 1:2, :])
            before = j > me if reverse else j < me
            grown = cmul(enter, decay)
            enter = (
                jnp.where(before, grown[0] + piece[0], enter[0]),
                jnp.where(before, grown[1] + piece[1], enter[1]),
            )
            grown = cmul(whole, decay)
            whole = (grown[0] + piece[0], grown[1] + piece[1])
            grown = cmul(power, decay)
            power = (
                jnp.where(before, grown[0], power[0]),
                jnp.where(before, grown[1], power[1]),
            )
        return enter, whole, power

    def summed(pair, table_re, table_im, sign):
        tr, ti = table_re[...], sign * table_im[...]
        re, im = cmul(pair, (tr, ti))
        return jnp.sum(re, axis=0, keepdims=True), jnp.sum(im, axis=0, keepdims=True)

    def put(ref, pair):
        ref[0:1, :] = pair[0]
        ref[1:2, :] = pair[1]

    push = (dot(x, bre[...]), dot(x, bim[...]))
    final = summed(push, v_re, v_im, 1.0)
    put(f_own, final)
    send(FWD_Y, "y", lambda j: f_own, f_recv.at[y], f_recv.at[0 : ny - 1])
    put(f_recv.at[y], final)
    local = scan_rows(push, dec, False)
    arrive(FWD_Y, "y", f_recv.at[0 : ny - 1])
    enter_y, whole_y, power_y = carried(f_recv, ny, y, dec_chunk, False)
    put(t_own, whole_y)
    send(FWD_Z, "z", lambda j: t_own, t_recv.at[z], t_recv.at[0 : nz - 1])
    put(t_recv.at[z], whole_y)

    gathered(OUT_A2, OUT_B2, wa_out, wb_out)
    project(BACK, cot, wa_out, wb_out, b_send, b_recv)

    arrive(FWD_Z, "z", t_recv.at[0 : nz - 1])
    enter_z, _, _ = carried(t_recv, nz, z, dec_row, False)
    far = cmul(power_y, enter_z)
    start = cmul(dec, (enter_y[0] + far[0], enter_y[1] + far[1]))
    add = cmul((u_re[...], u_im[...]), start)
    state_re, state_im = (local[0] + add[0]).astype(BF16), (local[1] + add[1]).astype(BF16)
    mixed = dot(state_re, cre[...], NT) - dot(state_im, cim[...], NT) + gain * x.astype(F32)
    c0 = math.sqrt(2.0 / math.pi)
    sq = mixed * mixed
    th = jnp.tanh(c0 * mixed * (1.0 + 0.044715 * sq))
    half_up = 0.5 * (1.0 + th)
    gated = (mixed * half_up).astype(BF16)
    slope = half_up + 0.5 * mixed * (1.0 - th * th) * (c0 * (1.0 + 3.0 * 0.044715 * sq))
    gat_own[...] = gated
    send(GATED, "d", lambda j: gat_own, gat_all.at[dp], gat_all.at[0 : nd - 1])
    gat_all[dp] = gated

    arrive(BACK, "d", b_recv.at[0 : nd - 1])
    inner = slope * total(b_recv).astype(F32)
    inner_b = inner.astype(BF16)
    pulled = (dot(inner_b, cre[...]), -dot(inner_b, cim[...]))
    opening = summed(pulled, u_re, u_im, -1.0)
    put(a_own, opening)
    send(BWD_Y, "y", lambda j: a_own, a_recv.at[y], a_recv.at[0 : ny - 1])
    put(a_recv.at[y], opening)
    back_dec = conj(dec)
    local = scan_rows(pulled, back_dec, True)
    arrive(BWD_Y, "y", a_recv.at[0 : ny - 1])
    enter_y, whole_y, power_y = carried(a_recv, ny, y, conj(dec_chunk), True)
    put(q_own, whole_y)
    send(BWD_Z, "z", lambda j: q_own, q_recv.at[z], q_recv.at[0 : nz - 1])
    put(q_recv.at[z], whole_y)

    def weight_grad(phase_a, phase_b, b, cols, act, sa, sb, ra, rb):
        part = dot(cols[b], act[...], TN).astype(BF16)
        sa[b] = part[:, 0:half].reshape(ny, per_group, half)
        sb[:, b] = part[:, half:].reshape(ny, per_group, half)

        @pl.when(b != z)
        def _():
            copy(phase_a, "z", b, sa.at[b], ra.at[z]).start()

        @pl.when(b == z)
        def _():
            ra[z] = sa[z]

        for k in ring_order(ny, True):
            j = peer("y", k)
            copy(phase_b, "y", j, sb.at[j, b], rb.at[y, b]).start()

    def all_blocks_sent(phase_a, phase_b, sb, ra, rb):
        rb[y] = sb[y]
        sent.append((phase_a, "z", ra.at[0 : nz - 1]))
        sent.append((phase_b, "y", rb.at[0 : ny - 1]))

    def reduced(recv, n):
        s = recv[0].astype(F32)
        for j in range(1, n):
            s = s + recv[j].astype(F32)
        return s

    def second_step(phase_a1, phase_b1, phase_a2, phase_b2, ra, rb, s2a, s2b, r2a, r2b):
        arrive(phase_a1, "z", ra.at[0 : nz - 1])
        s2a[...] = reduced(ra, nz).astype(BF16)
        send(phase_a2, "y", lambda j: s2a.at[j], r2a.at[y], r2a.at[0 : ny - 1])
        r2a[y] = s2a[y]
        arrive(phase_b1, "y", rb.at[0 : ny - 1])
        s2b[...] = reduced(rb, ny).astype(BF16)
        send(phase_b2, "z", lambda j: s2b.at[j], r2b.at[z], r2b.at[0 : nz - 1])
        r2b[z] = s2b[z]

    scale = (rows * ny * nz) ** -0.5

    def finish(phase_a2, phase_b2, r2a, r2b, out):
        arrive(phase_a2, "y", r2a.at[0 : ny - 1])
        arrive(phase_b2, "z", r2b.at[0 : nz - 1])
        out[:, 0:half] = reduced(r2a, ny) * scale
        out[:, half:] = reduced(r2b, nz) * scale

    arrive(GATED, "d", gat_all.at[0 : nd - 1])
    for b in range(nd):
        weight_grad(GO_A1, GO_B1, b, gat_all, cot, go_sa, go_sb, go_ra, go_rb)
    all_blocks_sent(GO_A1, GO_B1, go_sb, go_ra, go_rb)

    arrive(BWD_Z, "z", q_recv.at[0 : nz - 1])
    enter_z, _, _ = carried(q_recv, nz, z, conj(dec_row), True)
    far = cmul(power_y, enter_z)
    start = cmul(back_dec, (enter_y[0] + far[0], enter_y[1] + far[1]))
    add = cmul((v_re[...], -v_im[...]), start)
    adj_re, adj_im = (local[0] + add[0]).astype(BF16), (local[1] + add[1]).astype(BF16)
    mix = (dot(adj_re, bre[...], NT) + dot(adj_im, bim[...], NT) + gain * inner).astype(BF16)
    mix_own[...] = mix
    send(MIX, "d", lambda j: mix_own, mix_all.at[dp], mix_all.at[0 : nd - 1], lambda k: mix_sem.at[k])
    mix_all[dp] = mix

    weight_grad(GI_A1, GI_B1, dp, mix_all, tok, gi_sa, gi_sb, gi_ra, gi_rb)
    for k in ring_order(nd, False):
        j = peer("d", nd - k)
        copy(MIX, "d", j, mix_own, mix_all.at[j], mix_sem.at[k]).wait_recv()
        weight_grad(GI_A1, GI_B1, j, mix_all, tok, gi_sa, gi_sb, gi_ra, gi_rb)
    all_blocks_sent(GI_A1, GI_B1, gi_sb, gi_ra, gi_rb)
    second_step(GO_A1, GO_B1, GO_A2, GO_B2, go_ra, go_rb, go_s2a, go_s2b, go_r2a, go_r2b)
    grad = dot(mix_all[0], weights_of(wa_in, wb_in, 0))
    for b in range(1, nd):
        grad = grad + dot(mix_all[b], weights_of(wa_in, wb_in, b))
    o_tok[...] = grad.astype(BF16)
    second_step(GI_A1, GI_B1, GI_A2, GI_B2, gi_ra, gi_rb, gi_s2a, gi_s2b, gi_r2a, gi_r2b)
    finish(GO_A2, GO_B2, go_r2a, go_r2b, o_out)
    finish(GI_A2, GI_B2, gi_r2a, gi_r2b, o_in)

    @pl.when(z == dp)
    def _():
        param_copy(PK_Z, 1, pk_y.at[0 : nz - 1], pk_y.at[0 : nz - 1]).wait_send()
        param_copy(AUX_Z, 1, aux_y.at[0 : nz - 1], aux_y.at[0 : nz - 1]).wait_send()

    for phase, axis, whole in sent:
        copy(phase, axis, peer(axis, 1), whole, whole).wait_send()


def on_device(ny, nz, nd, tok, cot, win, wout, rate, freq, slog, dr, di, rr, ri, skip):
    rows, cols = tok.shape
    half = cols // 2
    states, c = rate.shape[1], skip.shape[1]
    own_ch, lanes, four = ny * c, ny * states, 4 * states
    V = pltpu.VMEM
    grads = [
        V((nz, ny, c, half), BF16), V((ny, nz, c, half), BF16),
        V((nz, ny, c, half), BF16), V((ny, nz, c, half), BF16),
        V((ny, c, half), BF16), V((nz, c, half), BF16),
        V((ny, c, half), BF16), V((nz, c, half), BF16),
    ]
    most = max(ny, nz, nd)
    vm = pl.BlockSpec(memory_space=pltpu.VMEM)
    drive = [jnp.swapaxes(a, 1, 2) for a in (dr, di)]
    args = (tok, cot, win, wout, rate, freq, *drive, rr, ri, skip)
    return pl.pallas_call(
        functools.partial(kernel, ny, nz, nd),
        out_shape=(
            jax.ShapeDtypeStruct((rows, cols), BF16),
            jax.ShapeDtypeStruct(win.shape, F32),
            jax.ShapeDtypeStruct(wout.shape, F32),
        ),
        in_specs=[pl.BlockSpec(memory_space=pltpu.SMEM)] + [pl.BlockSpec(memory_space=pltpu.HBM)] * len(args),
        out_specs=(vm, vm, vm),
        scratch_shapes=[
            *[V(a.shape, a.dtype) for a in args],
            V((c, four), BF16), V((8, lanes), F32),
            V((c, four), BF16), V((8, lanes), F32),
            V((ny, c, four), BF16), V((ny, 8, lanes), F32),
            V((nz, ny, c, half), BF16), V((ny, nz, c, half), BF16),
            V((nz, ny, c, half), BF16), V((ny, nz, c, half), BF16),
            V((nd, rows, own_ch), BF16), V((nd, rows, own_ch), BF16),
            V((nd, rows, own_ch), BF16), V((nd, rows, own_ch), BF16),
            V((2, lanes), F32), V((ny, 2, lanes), F32),
            V((2, lanes), F32), V((nz, 2, lanes), F32),
            V((2, lanes), F32), V((ny, 2, lanes), F32),
            V((2, lanes), F32), V((nz, 2, lanes), F32),
            V((rows, own_ch), BF16), V((nd, rows, own_ch), BF16),
            V((rows, own_ch), BF16), V((nd, rows, own_ch), BF16),
            *grads, *grads,
            *[V((own_ch, lanes), BF16)] * 4,
            *[V((rows, lanes), F32)] * 4,
            pltpu.SemaphoreType.DMA((PHASES,)),
            pltpu.SemaphoreType.DMA((PHASES,)),
            pltpu.SemaphoreType.DMA((2, most)),
            pltpu.SemaphoreType.DMA((nd,)),
            pltpu.SemaphoreType.DMA((len(args),)),
        ],
        compiler_params=pltpu.CompilerParams(
            collective_id=0, has_side_effects=True, vmem_limit_bytes=48 * 1024 * 1024
        ),
        name="mixer",
    )(slog, *[pltpu.with_memory_space_constraint(a, pltpu.HBM) for a in args])


def solution(mesh):
    nd = mesh.shape["dp"]
    nz = nd
    ny = mesh.shape["sp"] // nz
    return jax.shard_map(
        functools.partial(on_device, ny, nz, nd),
        mesh=mesh,
        in_specs=(
            P("sp", "dp"), P("sp", "dp"), P("sp", "dp"), P("sp", "dp"),
            P("sp", None), P("sp", None), P("sp"),
            P("sp", None, None), P("sp", None, None), P("sp", None, None), P("sp", None, None),
            P("sp", None),
        ),
        out_specs=(P("sp", "dp"), P("sp", "dp"), P("sp", "dp")),
        check_vma=False,
    )
```

```python
import functools
import math

import jax
import jax.numpy as jnp
from jax import lax
from jax.experimental import pallas as pl
from jax.experimental.pallas import tpu as pltpu
from jax.sharding import PartitionSpec as P

MESH = pl.DeviceIdType.MESH
F32 = jnp.float32
BF16 = jnp.bfloat16
HIGHEST = lax.Precision.HIGHEST

(
    IN_A1, IN_B1, IN_A2, IN_B2, OUT_A1, OUT_B1, OUT_A2, OUT_B2,
    PK_Z, AUX_Z, PK_Y, AUX_Y, DRIVE, BACK, FWD_Y, FWD_Z, BWD_Y, BWD_Z,
    GATED, MIX, GO_A1, GO_B1, GO_A2, GO_B2, GI_A1, GI_B1, GI_A2, GI_B2, GO_HA, GO_HB, GI_HA, GI_HB,
) = range(32)
PHASES = 32

NN = (((1,), (0,)), ((), ()))
NT = (((1,), (1,)), ((), ()))
TN = (((0,), (0,)), ((), ()))


def dot(a, b, dims=NN, precision=None):
    return lax.dot_general(a, b, dims, precision=precision, preferred_element_type=F32)


def cmul(a, b):
    return a[0] * b[0] - a[1] * b[1], a[0] * b[1] + a[1] * b[0]


def conj(a):
    return a[0], -a[1]


def square(a, times):
    for _ in range(times):
        a = (a[0] * a[0] - a[1] * a[1], 2.0 * a[0] * a[1])
    return a


def ring_order(n, far_first):
    ks = sorted(range(1, n), key=lambda k: (min(k, n - k), k))
    return ks[::-1] if far_first else ks


def slots(n):
    held = [0] + ring_order(n, False)
    return held, {k: i for i, k in enumerate(held)}


def slot_of(n, k):
    if n != 8:
        return k
    late = lax.div(k, 5)
    return (2 * k - 1) * (1 - late) + (16 - 2 * k) * late + 1 - lax.div(k + 7, 8)


def log2(n):
    return n.bit_length() - 1


def iota(shape, dim):
    return lax.broadcasted_iota(jnp.int32, shape, dim)


def scan_rows(pair, decay, reverse):
    re, im = pair
    rows, lanes = re.shape
    width = min(128, lanes)
    row = iota((rows, width), 0)
    outs = []
    for at in range(0, lanes, width):
        a, b = re[:, at : at + width], im[:, at : at + width]
        f = (decay[0][:, at : at + width], decay[1][:, at : at + width])
        for k in range(log2(rows)):
            step = 1 << k
            if reverse:
                turn, keep = rows - step, row < rows - step
            else:
                turn, keep = step, row >= step
            ra = jnp.where(keep, pltpu.roll(a, turn, 0), 0.0)
            rb = jnp.where(keep, pltpu.roll(b, turn, 0), 0.0)
            a, b = a + f[0] * ra - f[1] * rb, b + f[0] * rb + f[1] * ra
            f = square(f, 1)
        outs.append((a, b))
    return (
        jnp.concatenate([o[0] for o in outs], axis=1),
        jnp.concatenate([o[1] for o in outs], axis=1),
    )


def kernel(
    ny, nz, nd,
    slog, tok_h, cot_h, win_h, wout_h, rate_h, freq_h, dr_h, di_h, rr_h, ri_h, skip_h,
    o_tok, o_in, o_out,
    tok, cot, win, wout, rate, freq, dr, di, rr, ri, skip,
    pk_own, aux_own, pk_z, aux_z, pk_y, aux_y,
    wa_in, wb_in, wa_out, wb_out,
    d_send, d_recv, b_send, b_recv,
    f_own, f_recv, t_own, t_recv, a_own, a_recv, q_own, q_recv,
    gat_own, gat_all, mix_own, mix_all,
    go_sa, go_sb, go_ha, go_hb, go_ra, go_rb, go_s2a, go_s2b, go_r2a, go_r2b,
    gi_sa, gi_sb, gi_ha, gi_hb, gi_ra, gi_rb, gi_s2a, gi_s2b, gi_r2a, gi_r2b,
    bre, bim, cre, cim, u_re, u_im, v_re, v_im,
    ssem, rsem, in1_sem, in2_sem, mix_sem, load_sem,
):
    sp, dp = lax.axis_index("sp"), lax.axis_index("dp")
    z, y = lax.div(sp, ny), lax.rem(sp, ny)
    size = {"y": ny, "z": nz, "d": nd}
    here = {"y": y, "z": z, "d": dp}
    rows = tok.shape[0]
    states = rate.shape[1]
    per_group = skip.shape[1]
    own_ch = ny * per_group
    lanes = ny * states
    half = win.shape[1] // 2
    core = lax.rem(dp, 2)
    _, at_y = slots(ny)
    _, at_z = slots(nz)
    slot = {"y": lambda k: at_y[k % ny], "z": lambda k: at_z[k % nz]}

    def device(axis, j):
        if axis == "y":
            return (z * ny + j, dp)
        if axis == "z":
            return (j * ny + y, dp)
        return (sp, j)

    def peer(axis, k):
        return lax.rem(here[axis] + k, size[axis])

    def copy(phase, axis, j, src, dst, recv_sem=None):
        return pltpu.make_async_remote_copy(
            src_ref=src,
            dst_ref=dst,
            send_sem=ssem.at[phase],
            recv_sem=rsem.at[phase] if recv_sem is None else recv_sem,
            device_id=device(axis, j),
            device_id_type=MESH,
        )

    sent = []

    def send(phase, axis, src, dst, whole, sems=None):
        for k in ring_order(size[axis], True):
            copy(phase, axis, peer(axis, k), src(k), dst(k), None if sems is None else sems(k)).start()
        sent.append((phase, axis, whole))

    def arrive(phase, axis, whole):
        copy(phase, axis, peer(axis, 1), whole, whole).wait_recv()

    pairs = (
        (win_h, win), (wout_h, wout), (rate_h, rate), (freq_h, freq), (dr_h, dr), (di_h, di), (rr_h, rr),
        (ri_h, ri), (skip_h, skip), (tok_h, tok), (cot_h, cot),
    )
    loads = [pltpu.make_async_copy(a, b, load_sem.at[i]) for i, (a, b) in enumerate(pairs)]
    for load in loads:
        load.start()

    barrier = pltpu.get_barrier_semaphore()
    for axis in ("y", "z", "d"):
        for k in ring_order(size[axis], True):
            j = peer(axis, k)
            pl.semaphore_signal(barrier, inc=1, device_id=device(axis, j), device_id_type=MESH)

    pl.semaphore_wait(barrier, (ny - 1) + (nz - 1) + (nd - 1))

    for load in loads[:2]:
        load.wait()

    def parts(n):
        return ((0, 1), (1, 5), (5, 8)) if n == 8 else ((0, 1), (1, n))

    def part_of(n, at):
        return [a <= at < b for a, b in parts(n)].index(True)

    def spread(phase, axis, w, src, a, b, sems=None):
        for k in ring_order(size[axis], True):
            at = slot[axis](-k)
            dst = w.at[at, a] if b is None else w.at[at, a:b]
            copy(phase, axis, peer(axis, k), src, dst, None if sems is None else sems(at)).start()

    def gathered(phase, axis, w):
        arrive(phase, axis, w.at[1:])
        sent.append((phase, axis, w.at[1:]))

    left, right = win.at[:, 0:half], win.at[:, half:]
    send(
        IN_A1, "y", lambda k: left, lambda k: wa_in.at[0, at_y[-k % ny]], wa_in.at[0, 1:],
        lambda k: in1_sem.at[0, part_of(ny, at_y[-k % ny])],
    )
    send(
        IN_B1, "z", lambda k: right, lambda k: wb_in.at[0, at_z[-k % nz]], wb_in.at[0, 1:],
        lambda k: in1_sem.at[1, part_of(nz, at_z[-k % nz])],
    )
    spread(IN_A2, "z", wa_in, left, 0, None, lambda at: in2_sem.at[0, at])
    spread(IN_B2, "y", wb_in, right, 0, None, lambda at: in2_sem.at[1, 0])
    wa_in[0, 0] = win[:, 0:half]
    wb_in[0, 0] = win[:, half:]
    wa_out[0, 0] = wout[:, 0:half]
    wb_out[0, 0] = wout[:, half:]
    for load in loads[2:9]:
        load.wait()

    tile_s = (iota((states, lanes), 0) == lax.rem(iota((states, lanes), 1), states)).astype(F32)
    wide = lambda ref: dot(jnp.broadcast_to(ref[...], (8, states)), tile_s, precision=HIGHEST)
    rate_w, freq_w = wide(rate), wide(freq)
    step = jnp.exp(jnp.full((8, lanes), slog[0], F32))
    magnitude = jnp.exp(-rate_w * step)
    angle = freq_w * step
    dec_re, dec_im = magnitude * jnp.cos(angle), magnitude * jnp.sin(angle)
    modulus = rate_w * rate_w + freq_w * freq_w
    hold_re = (-rate_w * (dec_re - 1.0) + freq_w * dec_im) / modulus
    hold_im = (-freq_w * (dec_re - 1.0) - rate_w * dec_im) / modulus
    tile_c = (
        iota((per_group, lanes), 0) == lax.rem(iota((per_group, lanes), 1), per_group)
    ).astype(F32)
    skip_w = dot(jnp.broadcast_to(skip[...], (8, per_group)), tile_c, precision=HIGHEST)
    row8 = iota((8, lanes), 0)
    aux_own[...] = jnp.where(row8 == 0, dec_re, jnp.where(row8 == 1, dec_im, skip_w))
    four = 4 * states
    p_row, p_lane = iota((states, four), 0), iota((states, four), 1)
    hr, hi = hold_re[0:1, 0:states], hold_im[0:1, 0:states]
    hr = jnp.concatenate([hr] * 4, axis=1) if four > lanes else hold_re[0:1, 0:four]
    hi = jnp.concatenate([hi] * 4, axis=1) if four > lanes else hold_im[0:1, 0:four]
    first, second = p_lane == p_row, p_lane == p_row + states
    sel_r = jnp.where(first, hr, 0.0) + jnp.where(second, hi, 0.0)
    sel_i = jnp.where(first, -hi, 0.0) + jnp.where(second, hr, 0.0)
    sel_c = (p_lane == p_row + 2 * states).astype(F32)
    sel_d = (p_lane == p_row + 3 * states).astype(F32)
    pk_own[...] = (
        dot(dr[0], sel_r, NN, HIGHEST)
        + dot(di[0], sel_i, NN, HIGHEST)
        + dot(rr[0], sel_c, NN, HIGHEST)
        + dot(ri[0], sel_d, NN, HIGHEST)
    ).astype(BF16)

    def param_copy(phase, k, src, dst):
        return copy(phase, "z", peer("z", k), src, dst)

    @pl.when(z == dp)
    def _():
        for k in ring_order(nz, True):
            param_copy(PK_Z, k, pk_own, pk_z).start()
            param_copy(AUX_Z, k, aux_own, aux_z).start()
        pk_z[...] = pk_own[...]
        aux_z[...] = aux_own[...]

    def forward(part):
        if part < len(parts(ny)):
            a, b = parts(ny)[part]
            own = wa_in.at[0, a:b]
            copy(IN_A1, "y", peer("y", 1), own, own, in1_sem.at[0, part]).wait_recv()
            spread(IN_A2, "z", wa_in, own, a, b, lambda at: in2_sem.at[0, at])
        if part < len(parts(nz)):
            a, b = parts(nz)[part]
            own = wb_in.at[0, a:b]
            copy(IN_B1, "z", peer("z", 1), own, own, in1_sem.at[1, part]).wait_recv()
            spread(IN_B2, "y", wb_in, own, a, b, lambda at: in2_sem.at[1, part])

    forward(1)
    send(OUT_A1, "y", lambda k: wout.at[:, 0:half], lambda k: wa_out.at[0, at_y[-k % ny]], wa_out.at[0, 1:])
    send(OUT_B1, "z", lambda k: wout.at[:, half:], lambda k: wb_out.at[0, at_z[-k % nz]], wb_out.at[0, 1:])
    if max(ny, nz) > 2:
        forward(2)

    @pl.when(z != dp)
    def _():
        param_copy(PK_Z, 1, pk_z, pk_z).wait_recv()
        param_copy(AUX_Z, 1, aux_z, aux_z).wait_recv()

    send(PK_Y, "y", lambda k: pk_z, lambda k: pk_y.at[y], pk_y.at[1:])
    send(AUX_Y, "y", lambda k: aux_z, lambda k: aux_y.at[y], aux_y.at[1:])
    pk_y[y] = pk_z[...]
    aux_y[y] = aux_z[...]


    def weights_of(wa, wb, b):
        return weights_at(wa, wb, slot_of(nz, lax.rem(b - z + nz, nz)))

    def weights_at(wa, wb, at):
        place = [slot_of(ny, lax.rem(g - y + ny, ny)) for g in range(ny)]
        left = jnp.concatenate([wa[at, i] for i in place], axis=0)
        right = jnp.concatenate([wb[i, at] for i in place], axis=0)
        return jnp.concatenate([left, right], axis=1)

    def project(phase, act, wa, wb, out, recv):
        for k in ring_order(nd, True):
            j = peer("d", k)
            out[j] = dot(act[...], weights_of(wa, wb, j), NT).astype(BF16)
            copy(phase, "d", j, out.at[j], recv.at[dp]).start()
        sent.append((phase, "d", recv.at[0 : nd - 1]))
        recv[dp] = dot(act[...], weights_of(wa, wb, dp), NT).astype(BF16)

    for load in loads[9:]:
        load.wait()
    for at in range(nz):
        for part, (a, e) in enumerate(parts(nz)):
            if at == a:
                got = wb_in.at[1:, a:e]
                with jax.named_scope("IN_B%d" % at):
                    copy(IN_B2, "y", peer("y", 1), got, got, in2_sem.at[1, part]).wait_recv()
        if at:
            with jax.named_scope("IN_A%d" % at):
                copy(IN_A2, "z", peer("z", 1), wa_in.at[at], wa_in.at[at], in2_sem.at[0, at]).wait_recv()
        b = peer("z", slots(nz)[0][at])
        d_send[b] = dot(tok[...], weights_at(wa_in, wb_in, at), NT).astype(BF16)

        @pl.when(b != dp)
        def _():
            copy(DRIVE, "d", b, d_send.at[b], d_recv.at[dp]).start()

        @pl.when(b == dp)
        def _():
            d_recv[dp] = d_send[dp]

    sent.append((IN_A2, "z", wa_in.at[1:]))
    sent.append((IN_B2, "y", wb_in.at[1:]))
    sent.append((DRIVE, "d", d_recv.at[0 : nd - 1]))
    arrive(OUT_A1, "y", wa_out.at[0, 1:])
    spread(OUT_A2, "z", wa_out, wa_out.at[0, 0:ny], 0, ny)
    arrive(OUT_B1, "z", wb_out.at[0, 1:])
    spread(OUT_B2, "y", wb_out, wb_out.at[0, 0:nz], 0, nz)

    arrive(PK_Y, "y", pk_y.at[0 : ny - 1])
    arrive(AUX_Y, "y", aux_y.at[0 : ny - 1])
    packed = pk_y[...].reshape(own_ch, four)
    diag = lax.div(iota((own_ch, lanes), 0), per_group) == lax.div(iota((own_ch, lanes), 1), states)
    s_row, s_lane = iota((four, lanes), 0), lax.rem(iota((four, lanes), 1), states)
    for at, ref in enumerate((bre, bim, cre, cim)):
        spread = (s_row == s_lane + at * states).astype(F32).astype(BF16)
        ref[...] = jnp.where(diag, dot(packed, spread), 0.0).astype(BF16)
    group_of_lane = lax.div(iota((1, lanes), 1), states)
    group_of_ch = lax.div(iota((1, own_ch), 1), per_group)
    dec = (jnp.zeros((1, lanes), F32), jnp.zeros((1, lanes), F32))
    gain = jnp.zeros((1, own_ch), F32)
    for g in range(ny):
        dec = (
            jnp.where(group_of_lane == g, aux_y[g, 0:1, :], dec[0]),
            jnp.where(group_of_lane == g, aux_y[g, 1:2, :], dec[1]),
        )
        gain = jnp.where(group_of_ch == g, aux_y[g, 2:3, 0:own_ch], gain)
    row = iota((rows, lanes), 0)
    up = (jnp.ones((rows, lanes), F32), jnp.zeros((rows, lanes), F32))
    down = up
    factor = dec
    for k in range(log2(rows)):
        bit = lax.rem(lax.div(row, 1 << k), 2) == 1
        more = cmul(up, factor)
        up = (jnp.where(bit, more[0], up[0]), jnp.where(bit, more[1], up[1]))
        more = cmul(down, factor)
        down = (jnp.where(bit, down[0], more[0]), jnp.where(bit, down[1], more[1]))
        factor = square(factor, 1)
    u_re[...], u_im[...] = up
    v_re[...], v_im[...] = down
    dec_chunk = factor
    dec_row = square(dec_chunk, log2(ny))

    def total(recv):
        s = recv[0].astype(F32)
        for b in range(1, nd):
            s = s + recv[b].astype(F32)
        return s.astype(BF16)

    arrive(DRIVE, "d", d_recv.at[0 : nd - 1])
    x = total(d_recv)

    def carried(recv, n, me, decay, reverse):
        zero = jnp.zeros((1, lanes), F32)
        enter, whole, power = (zero, zero), (zero, zero), (zero + 1.0, zero)
        for i in range(n):
            j = n - 1 - i if reverse else i
            piece = (recv[j, 0:1, :], recv[j, 1:2, :])
            before = j > me if reverse else j < me
            grown = cmul(enter, decay)
            enter = (
                jnp.where(before, grown[0] + piece[0], enter[0]),
                jnp.where(before, grown[1] + piece[1], enter[1]),
            )
            grown = cmul(whole, decay)
            whole = (grown[0] + piece[0], grown[1] + piece[1])
            grown = cmul(power, decay)
            power = (
                jnp.where(before, grown[0], power[0]),
                jnp.where(before, grown[1], power[1]),
            )
        return enter, whole, power

    def summed(pair, table_re, table_im, sign):
        tr, ti = table_re[...], sign * table_im[...]
        re, im = cmul(pair, (tr, ti))
        return jnp.sum(re, axis=0, keepdims=True), jnp.sum(im, axis=0, keepdims=True)

    def put(ref, pair):
        ref[0:1, :] = pair[0]
        ref[1:2, :] = pair[1]

    push = (dot(x, bre[...]), dot(x, bim[...]))
    final = summed(push, v_re, v_im, 1.0)
    put(f_own, final)
    send(FWD_Y, "y", lambda k: f_own, lambda k: f_recv.at[y], f_recv.at[0 : ny - 1])
    put(f_recv.at[y], final)
    local = scan_rows(push, dec, False)
    gathered(OUT_A2, "z", wa_out)
    gathered(OUT_B2, "y", wb_out)
    project(BACK, cot, wa_out, wb_out, b_send, b_recv)

    arrive(FWD_Y, "y", f_recv.at[0 : ny - 1])
    enter_y, whole_y, power_y = carried(f_recv, ny, y, dec_chunk, False)
    put(t_own, whole_y)
    send(FWD_Z, "z", lambda k: t_own, lambda k: t_recv.at[z], t_recv.at[0 : nz - 1])
    put(t_recv.at[z], whole_y)

    arrive(FWD_Z, "z", t_recv.at[0 : nz - 1])
    enter_z, _, _ = carried(t_recv, nz, z, dec_row, False)
    far = cmul(power_y, enter_z)
    start = cmul(dec, (enter_y[0] + far[0], enter_y[1] + far[1]))
    add = cmul((u_re[...], u_im[...]), start)
    state_re, state_im = (local[0] + add[0]).astype(BF16), (local[1] + add[1]).astype(BF16)
    mixed = dot(state_re, cre[...], NT) - dot(state_im, cim[...], NT) + gain * x.astype(F32)
    c0 = math.sqrt(2.0 / math.pi)
    sq = mixed * mixed
    th = jnp.tanh(c0 * mixed * (1.0 + 0.044715 * sq))
    half_up = 0.5 * (1.0 + th)
    gated = (mixed * half_up).astype(BF16)
    slope = half_up + 0.5 * mixed * (1.0 - th * th) * (c0 * (1.0 + 3.0 * 0.044715 * sq))
    arrive(BACK, "d", b_recv.at[0 : nd - 1])
    inner = slope * total(b_recv).astype(F32)
    inner_b = inner.astype(BF16)
    pulled = (dot(inner_b, cre[...]), -dot(inner_b, cim[...]))
    opening = summed(pulled, u_re, u_im, -1.0)
    put(a_own, opening)
    send(BWD_Y, "y", lambda k: a_own, lambda k: a_recv.at[y], a_recv.at[0 : ny - 1])
    put(a_recv.at[y], opening)
    gat_own[...] = gated
    send(GATED, "d", lambda k: gat_own, lambda k: gat_all.at[dp], gat_all.at[0 : nd - 1])
    gat_all[dp] = gated
    back_dec = conj(dec)
    local = scan_rows(pulled, back_dec, True)
    arrive(BWD_Y, "y", a_recv.at[0 : ny - 1])
    enter_y, whole_y, power_y = carried(a_recv, ny, y, conj(dec_chunk), True)
    put(q_own, whole_y)
    send(BWD_Z, "z", lambda k: q_own, lambda k: q_recv.at[z], q_recv.at[0 : nz - 1])
    put(q_recv.at[z], whole_y)

    def block_of_grad(b, cols, act, sa, sb):
        part = dot(cols[b], act[...], TN).astype(BF16)
        sa[b] = part[:, 0:half].reshape(ny, per_group, half)
        sb[:, b] = part[:, half:].reshape(ny, per_group, half)

    def hand_on(phase, phase_h, axis, s, h, r):
        if size[axis] != 8:
            for k in ring_order(size[axis], True):
                copy(phase, axis, peer(axis, k), s.at[peer(axis, k)], r.at[slot[axis](-k)]).start()
            sent.append((phase, axis, r.at[1:]))
        else:
            copy(phase_h, axis, peer(axis, 2 + 4 * core), s.at[peer(axis, 4)], h.at[2]).start()
            copy(phase_h, axis, peer(axis, 1), s.at[peer(axis, 3)], h.at[0]).start()
            copy(phase_h, axis, peer(axis, 7), s.at[peer(axis, 5)], h.at[1]).start()
            copy(phase, axis, peer(axis, 1), s.at[peer(axis, 1)], r.at[1]).start()
            copy(phase, axis, peer(axis, 7), s.at[peer(axis, 7)], r.at[2]).start()
        r[0] = s[here[axis]]

    def add_to(s, j, part):
        s[j] = (s[j].astype(F32) + part.astype(F32)).astype(BF16)

    def pass_on(phase, phase_h, axis, s, h, r):
        if size[axis] == 8:
            arrive(phase_h, axis, h)
            add_to(s, peer(axis, 2), h[0])
            add_to(s, peer(axis, 6), h[1])
            add_to(s, peer(axis, 2 + 4 * core), h[2])
            copy(phase, axis, peer(axis, 2), s.at[peer(axis, 2)], r.at[3]).start()
            copy(phase, axis, peer(axis, 6), s.at[peer(axis, 6)], r.at[4]).start()
            sent.append((phase_h, axis, h))
            sent.append((phase, axis, r.at[1:]))

    def reduced(recv, n):
        s = recv[0].astype(F32)
        for j in range(1, n):
            s = s + recv[j].astype(F32)
        return s

    def second_step(phase_a1, phase_b1, phase_a2, phase_b2, ra, rb, s2a, s2b, r2a, r2b):
        arrive(phase_a1, "z", ra.at[1:])
        s2a[...] = reduced(ra, ra.shape[0]).astype(BF16)
        send(phase_a2, "y", lambda k: s2a.at[peer("y", k)], lambda k: r2a.at[at_y[-k % ny]], r2a.at[1:])
        r2a[0] = s2a[y]
        arrive(phase_b1, "y", rb.at[1:])
        s2b[...] = reduced(rb, rb.shape[0]).astype(BF16)
        send(phase_b2, "z", lambda k: s2b.at[peer("z", k)], lambda k: r2b.at[at_z[-k % nz]], r2b.at[1:])
        r2b[0] = s2b[z]

    scale = (rows * ny * nz) ** -0.5

    def finish(phase_a2, phase_b2, r2a, r2b, out):
        arrive(phase_a2, "y", r2a.at[0 : ny - 1])
        arrive(phase_b2, "z", r2b.at[0 : nz - 1])
        out[:, 0:half] = reduced(r2a, ny) * scale
        out[:, half:] = reduced(r2b, nz) * scale

    arrive(GATED, "d", gat_all.at[0 : nd - 1])
    for b in range(nd):
        block_of_grad(b, gat_all, cot, go_sa, go_sb)
    hand_on(GO_A1, GO_HA, "z", go_sa, go_ha, go_ra)
    hand_on(GO_B1, GO_HB, "y", go_sb, go_hb, go_rb)

    arrive(BWD_Z, "z", q_recv.at[0 : nz - 1])
    enter_z, _, _ = carried(q_recv, nz, z, conj(dec_row), True)
    far = cmul(power_y, enter_z)
    start = cmul(back_dec, (enter_y[0] + far[0], enter_y[1] + far[1]))
    add = cmul((v_re[...], -v_im[...]), start)
    adj_re, adj_im = (local[0] + add[0]).astype(BF16), (local[1] + add[1]).astype(BF16)
    mix = (dot(adj_re, bre[...], NT) + dot(adj_im, bim[...], NT) + gain * inner).astype(BF16)
    mix_own[...] = mix
    send(MIX, "d", lambda k: mix_own, lambda k: mix_all.at[dp], mix_all.at[0 : nd - 1], lambda k: mix_sem.at[k])
    mix_all[dp] = mix

    pass_on(GO_A1, GO_HA, "z", go_sa, go_ha, go_ra)
    pass_on(GO_B1, GO_HB, "y", go_sb, go_hb, go_rb)
    block_of_grad(dp, mix_all, tok, gi_sa, gi_sb)
    for k in ring_order(nd, False):
        j = peer("d", nd - k)
        copy(MIX, "d", j, mix_own, mix_all.at[j], mix_sem.at[k]).wait_recv()
        block_of_grad(j, mix_all, tok, gi_sa, gi_sb)
    hand_on(GI_A1, GI_HA, "z", gi_sa, gi_ha, gi_ra)
    hand_on(GI_B1, GI_HB, "y", gi_sb, gi_hb, gi_rb)
    second_step(GO_A1, GO_B1, GO_A2, GO_B2, go_ra, go_rb, go_s2a, go_s2b, go_r2a, go_r2b)
    grad = dot(mix_all[0], weights_of(wa_in, wb_in, 0))
    for b in range(1, nd):
        grad = grad + dot(mix_all[b], weights_of(wa_in, wb_in, b))
    o_tok[...] = grad.astype(BF16)
    pass_on(GI_A1, GI_HA, "z", gi_sa, gi_ha, gi_ra)
    pass_on(GI_B1, GI_HB, "y", gi_sb, gi_hb, gi_rb)
    second_step(GI_A1, GI_B1, GI_A2, GI_B2, gi_ra, gi_rb, gi_s2a, gi_s2b, gi_r2a, gi_r2b)
    finish(GO_A2, GO_B2, go_r2a, go_r2b, o_out)
    finish(GI_A2, GI_B2, gi_r2a, gi_r2b, o_in)

    @pl.when(z == dp)
    def _():
        param_copy(PK_Z, 1, pk_y.at[0 : nz - 1], pk_y.at[0 : nz - 1]).wait_send()
        param_copy(AUX_Z, 1, aux_y.at[0 : nz - 1], aux_y.at[0 : nz - 1]).wait_send()

    for phase, axis, whole in sent:
        copy(phase, axis, peer(axis, 1), whole, whole).wait_send()


def store(a, b, c, out_a, out_b, out_c, sem):
    copies = [pltpu.make_async_copy(s, d, sem.at[i]) for i, (s, d) in enumerate(((a, out_a), (b, out_b), (c, out_c)))]
    for copy in copies:
        copy.start()
    for copy in copies:
        copy.wait()


def on_device(ny, nz, nd, tok, cot, win, wout, rate, freq, slog, dr, di, rr, ri, skip):
    rows, cols = tok.shape
    half = cols // 2
    states, c = rate.shape[1], skip.shape[1]
    own_ch, lanes, four = ny * c, ny * states, 4 * states
    V = pltpu.VMEM
    come = lambda n: 5 if n == 8 else n
    relayed = [
        V((nz, ny, c, half), BF16), V((ny, nz, c, half), BF16),
        V((3, ny, c, half), BF16), V((3, nz, c, half), BF16),
        V((come(nz), ny, c, half), BF16), V((come(ny), nz, c, half), BF16),
        V((ny, c, half), BF16), V((nz, c, half), BF16),
        V((ny, c, half), BF16), V((nz, c, half), BF16),
    ]
    vm = pl.BlockSpec(memory_space=pltpu.VMEM)
    drive = [jnp.swapaxes(a, 1, 2) for a in (dr, di)]
    args = (tok, cot, win, wout, rate, freq, *drive, rr, ri, skip)
    outs = pl.pallas_call(
        functools.partial(kernel, ny, nz, nd),
        out_shape=(
            jax.ShapeDtypeStruct((rows, cols), BF16),
            jax.ShapeDtypeStruct(win.shape, F32),
            jax.ShapeDtypeStruct(wout.shape, F32),
        ),
        in_specs=[pl.BlockSpec(memory_space=pltpu.SMEM)] + [pl.BlockSpec(memory_space=pltpu.HBM)] * len(args),
        out_specs=(vm, vm, vm),
        scratch_shapes=[
            *[V(a.shape, a.dtype) for a in args],
            V((c, four), BF16), V((8, lanes), F32),
            V((c, four), BF16), V((8, lanes), F32),
            V((ny, c, four), BF16), V((ny, 8, lanes), F32),
            V((nz, ny, c, half), BF16), V((ny, nz, c, half), BF16),
            V((nz, ny, c, half), BF16), V((ny, nz, c, half), BF16),
            V((nd, rows, own_ch), BF16), V((nd, rows, own_ch), BF16),
            V((nd, rows, own_ch), BF16), V((nd, rows, own_ch), BF16),
            V((2, lanes), F32), V((ny, 2, lanes), F32),
            V((2, lanes), F32), V((nz, 2, lanes), F32),
            V((2, lanes), F32), V((ny, 2, lanes), F32),
            V((2, lanes), F32), V((nz, 2, lanes), F32),
            V((rows, own_ch), BF16), V((nd, rows, own_ch), BF16),
            V((rows, own_ch), BF16), V((nd, rows, own_ch), BF16),
            *relayed, *relayed,
            *[V((own_ch, lanes), BF16)] * 4,
            *[V((rows, lanes), F32)] * 4,
            pltpu.SemaphoreType.DMA((PHASES,)),
            pltpu.SemaphoreType.DMA((PHASES,)),
            pltpu.SemaphoreType.DMA((2, 3)),
            pltpu.SemaphoreType.DMA((2, 8)),
            pltpu.SemaphoreType.DMA((nd,)),
            pltpu.SemaphoreType.DMA((len(args),)),
        ],
        compiler_params=pltpu.CompilerParams(
            collective_id=0, has_side_effects=True, vmem_limit_bytes=48 * 1024 * 1024
        ),
        name="mixer",
    )(slog, *[pltpu.with_memory_space_constraint(a, pltpu.HBM) for a in args])
    return pl.pallas_call(
        store,
        out_shape=tuple(jax.ShapeDtypeStruct(o.shape, o.dtype) for o in outs),
        in_specs=[vm] * 3,
        out_specs=(pl.BlockSpec(memory_space=pltpu.HBM),) * 3,
        scratch_shapes=[pltpu.SemaphoreType.DMA((3,))],
        compiler_params=pltpu.CompilerParams(vmem_limit_bytes=8 * 1024 * 1024),
        name="store",
    )(*outs)


def solution(mesh):
    nd = mesh.shape["dp"]
    nz = nd
    ny = mesh.shape["sp"] // nz
    return jax.shard_map(
        functools.partial(on_device, ny, nz, nd),
        mesh=mesh,
        in_specs=(
            P("sp", "dp"), P("sp", "dp"), P("sp", "dp"), P("sp", "dp"),
            P("sp", None), P("sp", None), P("sp"),
            P("sp", None, None), P("sp", None, None), P("sp", None, None), P("sp", None, None),
            P("sp", None),
        ),
        out_specs=(P("sp", "dp"), P("sp", "dp"), P("sp", "dp")),
        check_vma=False,
    )
```

```python
import functools
import math

import jax
import jax.numpy as jnp
from jax import lax
from jax.experimental import pallas as pl
from jax.experimental.pallas import tpu as pltpu
from jax.sharding import PartitionSpec as P

MESH = pl.DeviceIdType.MESH
F32 = jnp.float32
BF16 = jnp.bfloat16
HIGHEST = lax.Precision.HIGHEST

(
    IN_A1, IN_B1, IN_A2, IN_B2, OUT_A1, OUT_B1, OUT_A2, OUT_B2,
    PK_Z, AUX_Z, PK_Y, AUX_Y, DRIVE, BACK, FWD_Y, FWD_Z, BWD_Y, BWD_Z,
    GATED, MIX, GO_A1, GO_B1, GO_A2, GO_B2, GI_A1, GI_B1, GI_A2, GI_B2, GO_HA, GO_HB, GI_HA, GI_HB,
) = range(32)
PHASES = 32

NN = (((1,), (0,)), ((), ()))
NT = (((1,), (1,)), ((), ()))
TN = (((0,), (0,)), ((), ()))


def dot(a, b, dims=NN, precision=None):
    return lax.dot_general(a, b, dims, precision=precision, preferred_element_type=F32)


def cmul(a, b):
    return a[0] * b[0] - a[1] * b[1], a[0] * b[1] + a[1] * b[0]


def conj(a):
    return a[0], -a[1]


def square(a, times):
    for _ in range(times):
        a = (a[0] * a[0] - a[1] * a[1], 2.0 * a[0] * a[1])
    return a


def ring_order(n, far_first):
    ks = sorted(range(1, n), key=lambda k: (min(k, n - k), k))
    return ks[::-1] if far_first else ks


def slots(n):
    held = [0] + ring_order(n, False)
    return held, {k: i for i, k in enumerate(held)}


def slot_of(n, k):
    if n != 8:
        return k
    late = lax.div(k, 5)
    return (2 * k - 1) * (1 - late) + (16 - 2 * k) * late + 1 - lax.div(k + 7, 8)


def log2(n):
    return n.bit_length() - 1


def iota(shape, dim):
    return lax.broadcasted_iota(jnp.int32, shape, dim)


def scan_rows(pair, decay, reverse):
    re, im = pair
    rows, lanes = re.shape
    width = min(128, lanes)
    row = iota((rows, width), 0)
    outs = []
    for at in range(0, lanes, width):
        a, b = re[:, at : at + width], im[:, at : at + width]
        f = (decay[0][:, at : at + width], decay[1][:, at : at + width])
        for k in range(log2(rows)):
            step = 1 << k
            if reverse:
                turn, keep = rows - step, row < rows - step
            else:
                turn, keep = step, row >= step
            ra = jnp.where(keep, pltpu.roll(a, turn, 0), 0.0)
            rb = jnp.where(keep, pltpu.roll(b, turn, 0), 0.0)
            a, b = a + f[0] * ra - f[1] * rb, b + f[0] * rb + f[1] * ra
            f = square(f, 1)
        outs.append((a, b))
    return (
        jnp.concatenate([o[0] for o in outs], axis=1),
        jnp.concatenate([o[1] for o in outs], axis=1),
    )


def kernel(
    ny, nz, nd,
    slog, tok_h, cot_h, win_h, wout_h, rate_h, freq_h, dr_h, di_h, rr_h, ri_h, skip_h,
    o_tok, o_in, o_out,
    tok, cot, win, wout, rate, freq, dr, di, rr, ri, skip,
    pk_own, aux_own, pk_z, aux_z, pk_y, aux_y,
    wa_in, wb_in, wa_out, wb_out,
    d_send, d_recv, b_send, b_recv,
    f_own, f_recv, a_own, a_recv, w_re, w_im,
    gat_own, gat_all, mix_own, mix_all,
    go_sa, go_sb, go_ha, go_hb, go_ra, go_rb, go_s2a, go_s2b, go_r2a, go_r2b,
    gi_sa, gi_sb, gi_ha, gi_hb, gi_ra, gi_rb, gi_s2a, gi_s2b, gi_r2a, gi_r2b,
    bre, bim, cre, cim, u_re, u_im, v_re, v_im,
    ssem, rsem, in1_sem, in2_sem, mix_sem, load_sem,
):
    sp, dp = lax.axis_index("sp"), lax.axis_index("dp")
    z, y = lax.div(sp, ny), lax.rem(sp, ny)
    size = {"y": ny, "z": nz, "d": nd}
    here = {"y": y, "z": z, "d": dp}
    rows = tok.shape[0]
    states = rate.shape[1]
    per_group = skip.shape[1]
    own_ch = ny * per_group
    lanes = ny * states
    half = win.shape[1] // 2
    core = lax.rem(dp, 2)
    _, at_y = slots(ny)
    _, at_z = slots(nz)
    slot = {"y": lambda k: at_y[k % ny], "z": lambda k: at_z[k % nz]}

    def device(axis, j):
        if axis == "y":
            return (z * ny + j, dp)
        if axis == "z":
            return (j * ny + y, dp)
        return (sp, j)

    def peer(axis, k):
        return lax.rem(here[axis] + k, size[axis])

    def copy(phase, axis, j, src, dst, recv_sem=None):
        return pltpu.make_async_remote_copy(
            src_ref=src,
            dst_ref=dst,
            send_sem=ssem.at[phase],
            recv_sem=rsem.at[phase] if recv_sem is None else recv_sem,
            device_id=device(axis, j),
            device_id_type=MESH,
        )

    sent = []

    def send(phase, axis, src, dst, whole, sems=None):
        for k in ring_order(size[axis], True):
            copy(phase, axis, peer(axis, k), src(k), dst(k), None if sems is None else sems(k)).start()
        sent.append((phase, axis, whole))

    def arrive(phase, axis, whole):
        copy(phase, axis, peer(axis, 1), whole, whole).wait_recv()

    pairs = (
        (win_h, win), (wout_h, wout), (rate_h, rate), (freq_h, freq), (dr_h, dr), (di_h, di), (rr_h, rr),
        (ri_h, ri), (skip_h, skip), (tok_h, tok), (cot_h, cot),
    )
    loads = [pltpu.make_async_copy(a, b, load_sem.at[i]) for i, (a, b) in enumerate(pairs)]
    for load in loads:
        load.start()

    barrier = pltpu.get_barrier_semaphore()
    for axis in ("y", "z", "d"):
        for k in ring_order(size[axis], True):
            j = peer(axis, k)
            pl.semaphore_signal(barrier, inc=1, device_id=device(axis, j), device_id_type=MESH)

    pl.semaphore_wait(barrier, (ny - 1) + (nz - 1) + (nd - 1))

    for load in loads[:2]:
        load.wait()

    def parts(n):
        return ((0, 1), (1, 5), (5, 8)) if n == 8 else ((0, 1), (1, n))

    def part_of(n, at):
        return [a <= at < b for a, b in parts(n)].index(True)

    def spread(phase, axis, w, src, a, b, sems=None):
        for k in ring_order(size[axis], True):
            at = slot[axis](-k)
            dst = w.at[at, a] if b is None else w.at[at, a:b]
            copy(phase, axis, peer(axis, k), src, dst, None if sems is None else sems(at)).start()

    def gathered(phase, axis, w):
        arrive(phase, axis, w.at[1:])
        sent.append((phase, axis, w.at[1:]))

    left, right = win.at[:, 0:half], win.at[:, half:]
    send(
        IN_A1, "y", lambda k: left, lambda k: wa_in.at[0, at_y[-k % ny]], wa_in.at[0, 1:],
        lambda k: in1_sem.at[0, part_of(ny, at_y[-k % ny])],
    )
    send(
        IN_B1, "z", lambda k: right, lambda k: wb_in.at[0, at_z[-k % nz]], wb_in.at[0, 1:],
        lambda k: in1_sem.at[1, part_of(nz, at_z[-k % nz])],
    )
    spread(IN_A2, "z", wa_in, left, 0, None, lambda at: in2_sem.at[0, at])
    spread(IN_B2, "y", wb_in, right, 0, None, lambda at: in2_sem.at[1, 0])
    wa_in[0, 0] = win[:, 0:half]
    wb_in[0, 0] = win[:, half:]
    wa_out[0, 0] = wout[:, 0:half]
    wb_out[0, 0] = wout[:, half:]
    for load in loads[2:9]:
        load.wait()

    tile_s = (iota((states, lanes), 0) == lax.rem(iota((states, lanes), 1), states)).astype(F32)
    wide = lambda ref: dot(jnp.broadcast_to(ref[...], (8, states)), tile_s, precision=HIGHEST)
    rate_w, freq_w = wide(rate), wide(freq)
    step = jnp.exp(jnp.full((8, lanes), slog[0], F32))
    magnitude = jnp.exp(-rate_w * step)
    angle = freq_w * step
    dec_re, dec_im = magnitude * jnp.cos(angle), magnitude * jnp.sin(angle)
    modulus = rate_w * rate_w + freq_w * freq_w
    hold_re = (-rate_w * (dec_re - 1.0) + freq_w * dec_im) / modulus
    hold_im = (-freq_w * (dec_re - 1.0) - rate_w * dec_im) / modulus
    tile_c = (
        iota((per_group, lanes), 0) == lax.rem(iota((per_group, lanes), 1), per_group)
    ).astype(F32)
    skip_w = dot(jnp.broadcast_to(skip[...], (8, per_group)), tile_c, precision=HIGHEST)
    row8 = iota((8, lanes), 0)
    aux_own[...] = jnp.where(row8 == 0, dec_re, jnp.where(row8 == 1, dec_im, skip_w))
    four = 4 * states
    p_row, p_lane = iota((states, four), 0), iota((states, four), 1)
    hr, hi = hold_re[0:1, 0:states], hold_im[0:1, 0:states]
    hr = jnp.concatenate([hr] * 4, axis=1) if four > lanes else hold_re[0:1, 0:four]
    hi = jnp.concatenate([hi] * 4, axis=1) if four > lanes else hold_im[0:1, 0:four]
    first, second = p_lane == p_row, p_lane == p_row + states
    sel_r = jnp.where(first, hr, 0.0) + jnp.where(second, hi, 0.0)
    sel_i = jnp.where(first, -hi, 0.0) + jnp.where(second, hr, 0.0)
    sel_c = (p_lane == p_row + 2 * states).astype(F32)
    sel_d = (p_lane == p_row + 3 * states).astype(F32)
    pk_own[...] = (
        dot(dr[0], sel_r, NN, HIGHEST)
        + dot(di[0], sel_i, NN, HIGHEST)
        + dot(rr[0], sel_c, NN, HIGHEST)
        + dot(ri[0], sel_d, NN, HIGHEST)
    ).astype(BF16)

    def param_copy(phase, k, src, dst):
        return copy(phase, "z", peer("z", k), src, dst)

    @pl.when(z == dp)
    def _():
        for k in ring_order(nz, True):
            param_copy(PK_Z, k, pk_own, pk_z).start()
            param_copy(AUX_Z, k, aux_own, aux_z).start()
        pk_z[...] = pk_own[...]
        aux_z[...] = aux_own[...]

    def forward(part):
        if part < len(parts(ny)):
            a, b = parts(ny)[part]
            own = wa_in.at[0, a:b]
            copy(IN_A1, "y", peer("y", 1), own, own, in1_sem.at[0, part]).wait_recv()
            spread(IN_A2, "z", wa_in, own, a, b, lambda at: in2_sem.at[0, at])
        if part < len(parts(nz)):
            a, b = parts(nz)[part]
            own = wb_in.at[0, a:b]
            copy(IN_B1, "z", peer("z", 1), own, own, in1_sem.at[1, part]).wait_recv()
            spread(IN_B2, "y", wb_in, own, a, b, lambda at: in2_sem.at[1, part])

    forward(1)
    send(OUT_A1, "y", lambda k: wout.at[:, 0:half], lambda k: wa_out.at[0, at_y[-k % ny]], wa_out.at[0, 1:])
    send(OUT_B1, "z", lambda k: wout.at[:, half:], lambda k: wb_out.at[0, at_z[-k % nz]], wb_out.at[0, 1:])
    if max(ny, nz) > 2:
        forward(2)

    @pl.when(z != dp)
    def _():
        param_copy(PK_Z, 1, pk_z, pk_z).wait_recv()
        param_copy(AUX_Z, 1, aux_z, aux_z).wait_recv()

    send(PK_Y, "y", lambda k: pk_z, lambda k: pk_y.at[y], pk_y.at[1:])
    send(AUX_Y, "y", lambda k: aux_z, lambda k: aux_y.at[y], aux_y.at[1:])
    pk_y[y] = pk_z[...]
    aux_y[y] = aux_z[...]


    def weights_of(wa, wb, b):
        return weights_at(wa, wb, slot_of(nz, lax.rem(b - z + nz, nz)))

    def weights_at(wa, wb, at):
        place = [slot_of(ny, lax.rem(g - y + ny, ny)) for g in range(ny)]
        left = jnp.concatenate([wa[at, i] for i in place], axis=0)
        right = jnp.concatenate([wb[i, at] for i in place], axis=0)
        return jnp.concatenate([left, right], axis=1)

    def project(phase, act, wa, wb, out, recv):
        for k in ring_order(nd, True):
            j = peer("d", k)
            out[j] = dot(act[...], weights_of(wa, wb, j), NT).astype(BF16)
            copy(phase, "d", j, out.at[j], recv.at[dp]).start()
        sent.append((phase, "d", recv.at[0 : nd - 1]))
        recv[dp] = dot(act[...], weights_of(wa, wb, dp), NT).astype(BF16)

    for load in loads[9:]:
        load.wait()
    for at in range(nz):
        for part, (a, e) in enumerate(parts(nz)):
            if at == a:
                got = wb_in.at[1:, a:e]
                with jax.named_scope("IN_B%d" % at):
                    copy(IN_B2, "y", peer("y", 1), got, got, in2_sem.at[1, part]).wait_recv()
        if at:
            with jax.named_scope("IN_A%d" % at):
                copy(IN_A2, "z", peer("z", 1), wa_in.at[at], wa_in.at[at], in2_sem.at[0, at]).wait_recv()
        b = peer("z", slots(nz)[0][at])
        d_send[b] = dot(tok[...], weights_at(wa_in, wb_in, at), NT).astype(BF16)

        @pl.when(b != dp)
        def _():
            copy(DRIVE, "d", b, d_send.at[b], d_recv.at[dp]).start()

        @pl.when(b == dp)
        def _():
            d_recv[dp] = d_send[dp]

    sent.append((IN_A2, "z", wa_in.at[1:]))
    sent.append((IN_B2, "y", wb_in.at[1:]))
    sent.append((DRIVE, "d", d_recv.at[0 : nd - 1]))
    arrive(OUT_A1, "y", wa_out.at[0, 1:])
    spread(OUT_A2, "z", wa_out, wa_out.at[0, 0:ny], 0, ny)
    arrive(OUT_B1, "z", wb_out.at[0, 1:])
    spread(OUT_B2, "y", wb_out, wb_out.at[0, 0:nz], 0, nz)

    arrive(PK_Y, "y", pk_y.at[0 : ny - 1])
    arrive(AUX_Y, "y", aux_y.at[0 : ny - 1])
    packed = pk_y[...].reshape(own_ch, four)
    diag = lax.div(iota((own_ch, lanes), 0), per_group) == lax.div(iota((own_ch, lanes), 1), states)
    s_row, s_lane = iota((four, lanes), 0), lax.rem(iota((four, lanes), 1), states)
    for at, ref in enumerate((bre, bim, cre, cim)):
        spread = (s_row == s_lane + at * states).astype(F32).astype(BF16)
        ref[...] = jnp.where(diag, dot(packed, spread), 0.0).astype(BF16)
    group_of_lane = lax.div(iota((1, lanes), 1), states)
    group_of_ch = lax.div(iota((1, own_ch), 1), per_group)
    dec = (jnp.zeros((1, lanes), F32), jnp.zeros((1, lanes), F32))
    gain = jnp.zeros((1, own_ch), F32)
    for g in range(ny):
        dec = (
            jnp.where(group_of_lane == g, aux_y[g, 0:1, :], dec[0]),
            jnp.where(group_of_lane == g, aux_y[g, 1:2, :], dec[1]),
        )
        gain = jnp.where(group_of_ch == g, aux_y[g, 2:3, 0:own_ch], gain)
    row = iota((rows, lanes), 0)
    up = (jnp.ones((rows, lanes), F32), jnp.zeros((rows, lanes), F32))
    down = up
    factor = dec
    for k in range(log2(rows)):
        bit = lax.rem(lax.div(row, 1 << k), 2) == 1
        more = cmul(up, factor)
        up = (jnp.where(bit, more[0], up[0]), jnp.where(bit, more[1], up[1]))
        more = cmul(down, factor)
        down = (jnp.where(bit, down[0], more[0]), jnp.where(bit, down[1], more[1]))
        factor = square(factor, 1)
    u_re[...], u_im[...] = up
    v_re[...], v_im[...] = down
    dec_chunk = factor

    def total(recv):
        s = recv[0].astype(F32)
        for b in range(1, nd):
            s = s + recv[b].astype(F32)
        return s.astype(BF16)

    arrive(DRIVE, "d", d_recv.at[0 : nd - 1])
    x = total(d_recv)

    chunks = ny * nz

    def to_all(phase, own, recv, reverse):
        far = lambda k, n: min(k, n - k)
        offsets = [(a, b) for a in range(nz) for b in range(ny) if a or b]
        for a, b in sorted(offsets, key=lambda o: -far(o[0], nz) - far(o[1], ny)):
            j = peer("z", a) * ny + peer("y", b)
            ahead = sp - j if reverse else j - sp
            pltpu.make_async_remote_copy(
                src_ref=own,
                dst_ref=recv.at[lax.rem(ahead - 1 + 2 * chunks, chunks)],
                send_sem=ssem.at[phase],
                recv_sem=rsem.at[phase],
                device_id=(j, dp),
                device_id_type=MESH,
            ).start()
        sent.append((phase, "y", recv.at[1:]))

    def entering(recv, reverse):
        held = iota((chunks, 2, lanes), 0) < (chunks - 1 - sp if reverse else sp)
        state = jnp.where(held, recv[...], 0.0)
        by_re = jnp.sum(state * w_re[...], axis=0)
        by_im = jnp.sum(state * w_im[...], axis=0)
        if reverse:
            by_im = -by_im
        return by_re[0:1] - by_im[1:2], by_re[1:2] + by_im[0:1]

    def summed(pair, table_re, table_im, sign):
        tr, ti = table_re[...], sign * table_im[...]
        re, im = cmul(pair, (tr, ti))
        return jnp.sum(re, axis=0, keepdims=True), jnp.sum(im, axis=0, keepdims=True)

    def put(ref, pair):
        ref[0:1, :] = pair[0]
        ref[1:2, :] = pair[1]

    push = (dot(x, bre[...]), dot(x, bim[...]))
    final = summed(push, v_re, v_im, 1.0)
    put(f_own, final)
    to_all(FWD_Y, f_own, f_recv, False)
    local = scan_rows(push, dec, False)
    gathered(OUT_A2, "z", wa_out)
    gathered(OUT_B2, "y", wb_out)
    project(BACK, cot, wa_out, wb_out, b_send, b_recv)

    row = iota((chunks, lanes), 0)
    power, factor = (jnp.ones((chunks, lanes), F32), jnp.zeros((chunks, lanes), F32)), dec_chunk
    for k in range(log2(chunks)):
        bit = lax.rem(lax.div(row, 1 << k), 2) == 1
        more = cmul(power, factor)
        power = (jnp.where(bit, more[0], power[0]), jnp.where(bit, more[1], power[1]))
        factor = square(factor, 1)
    w_re[...] = jnp.broadcast_to(power[0][:, None, :], (chunks, 2, lanes))
    w_im[...] = jnp.broadcast_to(power[1][:, None, :], (chunks, 2, lanes))
    arrive(FWD_Y, "y", f_recv.at[1:])
    start = cmul(dec, entering(f_recv, False))
    add = cmul((u_re[...], u_im[...]), start)
    state_re, state_im = (local[0] + add[0]).astype(BF16), (local[1] + add[1]).astype(BF16)
    mixed = dot(state_re, cre[...], NT) - dot(state_im, cim[...], NT) + gain * x.astype(F32)
    c0 = math.sqrt(2.0 / math.pi)
    sq = mixed * mixed
    th = jnp.tanh(c0 * mixed * (1.0 + 0.044715 * sq))
    half_up = 0.5 * (1.0 + th)
    gated = (mixed * half_up).astype(BF16)
    slope = half_up + 0.5 * mixed * (1.0 - th * th) * (c0 * (1.0 + 3.0 * 0.044715 * sq))
    arrive(BACK, "d", b_recv.at[0 : nd - 1])
    inner = slope * total(b_recv).astype(F32)
    inner_b = inner.astype(BF16)
    pulled = (dot(inner_b, cre[...]), -dot(inner_b, cim[...]))
    opening = summed(pulled, u_re, u_im, -1.0)
    put(a_own, opening)
    to_all(BWD_Y, a_own, a_recv, True)
    gat_own[...] = gated
    send(GATED, "d", lambda k: gat_own, lambda k: gat_all.at[dp], gat_all.at[0 : nd - 1])
    gat_all[dp] = gated
    back_dec = conj(dec)
    local = scan_rows(pulled, back_dec, True)
    def block_of_grad(b, cols, act, sa, sb):
        part = dot(cols[b], act[...], TN).astype(BF16)
        sa[b] = part[:, 0:half].reshape(ny, per_group, half)
        sb[:, b] = part[:, half:].reshape(ny, per_group, half)

    def hand_on(phase, phase_h, axis, s, h, r):
        if size[axis] != 8:
            for k in ring_order(size[axis], True):
                copy(phase, axis, peer(axis, k), s.at[peer(axis, k)], r.at[slot[axis](-k)]).start()
            sent.append((phase, axis, r.at[1:]))
        else:
            copy(phase_h, axis, peer(axis, 2 + 4 * core), s.at[peer(axis, 4)], h.at[2]).start()
            copy(phase_h, axis, peer(axis, 1), s.at[peer(axis, 3)], h.at[0]).start()
            copy(phase_h, axis, peer(axis, 7), s.at[peer(axis, 5)], h.at[1]).start()
            copy(phase, axis, peer(axis, 1), s.at[peer(axis, 1)], r.at[1]).start()
            copy(phase, axis, peer(axis, 7), s.at[peer(axis, 7)], r.at[2]).start()
        r[0] = s[here[axis]]

    def add_to(s, j, part):
        s[j] = (s[j].astype(F32) + part.astype(F32)).astype(BF16)

    def pass_on(phase, phase_h, axis, s, h, r):
        if size[axis] == 8:
            arrive(phase_h, axis, h)
            add_to(s, peer(axis, 2), h[0])
            add_to(s, peer(axis, 6), h[1])
            add_to(s, peer(axis, 2 + 4 * core), h[2])
            copy(phase, axis, peer(axis, 2), s.at[peer(axis, 2)], r.at[3]).start()
            copy(phase, axis, peer(axis, 6), s.at[peer(axis, 6)], r.at[4]).start()
            sent.append((phase_h, axis, h))
            sent.append((phase, axis, r.at[1:]))

    def reduced(recv, n):
        s = recv[0].astype(F32)
        for j in range(1, n):
            s = s + recv[j].astype(F32)
        return s

    def second_step(phase_a1, phase_b1, phase_a2, phase_b2, ra, rb, s2a, s2b, r2a, r2b):
        arrive(phase_a1, "z", ra.at[1:])
        s2a[...] = reduced(ra, ra.shape[0]).astype(BF16)
        send(phase_a2, "y", lambda k: s2a.at[peer("y", k)], lambda k: r2a.at[at_y[-k % ny]], r2a.at[1:])
        r2a[0] = s2a[y]
        arrive(phase_b1, "y", rb.at[1:])
        s2b[...] = reduced(rb, rb.shape[0]).astype(BF16)
        send(phase_b2, "z", lambda k: s2b.at[peer("z", k)], lambda k: r2b.at[at_z[-k % nz]], r2b.at[1:])
        r2b[0] = s2b[z]

    scale = (rows * ny * nz) ** -0.5

    def finish(phase_a2, phase_b2, r2a, r2b, out):
        arrive(phase_a2, "y", r2a.at[0 : ny - 1])
        arrive(phase_b2, "z", r2b.at[0 : nz - 1])
        out[:, 0:half] = reduced(r2a, ny) * scale
        out[:, half:] = reduced(r2b, nz) * scale

    arrive(GATED, "d", gat_all.at[0 : nd - 1])
    for b in range(nd):
        block_of_grad(b, gat_all, cot, go_sa, go_sb)
    hand_on(GO_A1, GO_HA, "z", go_sa, go_ha, go_ra)
    hand_on(GO_B1, GO_HB, "y", go_sb, go_hb, go_rb)

    arrive(BWD_Y, "y", a_recv.at[1:])
    start = cmul(back_dec, entering(a_recv, True))
    add = cmul((v_re[...], -v_im[...]), start)
    adj_re, adj_im = (local[0] + add[0]).astype(BF16), (local[1] + add[1]).astype(BF16)
    mix = (dot(adj_re, bre[...], NT) + dot(adj_im, bim[...], NT) + gain * inner).astype(BF16)
    mix_own[...] = mix
    send(MIX, "d", lambda k: mix_own, lambda k: mix_all.at[dp], mix_all.at[0 : nd - 1], lambda k: mix_sem.at[k])
    mix_all[dp] = mix

    block_of_grad(dp, mix_all, tok, gi_sa, gi_sb)
    for i, k in enumerate(ring_order(nd, False)):
        j = peer("d", nd - k)
        copy(MIX, "d", j, mix_own, mix_all.at[j], mix_sem.at[k]).wait_recv()
        block_of_grad(j, mix_all, tok, gi_sa, gi_sb)
        if i == min(1, nd - 2):
            pass_on(GO_A1, GO_HA, "z", go_sa, go_ha, go_ra)
            pass_on(GO_B1, GO_HB, "y", go_sb, go_hb, go_rb)
    hand_on(GI_A1, GI_HA, "z", gi_sa, gi_ha, gi_ra)
    hand_on(GI_B1, GI_HB, "y", gi_sb, gi_hb, gi_rb)
    grad = dot(mix_all[0], weights_of(wa_in, wb_in, 0))
    for b in range(1, nd):
        grad = grad + dot(mix_all[b], weights_of(wa_in, wb_in, b))
    o_tok[...] = grad.astype(BF16)
    pass_on(GI_A1, GI_HA, "z", gi_sa, gi_ha, gi_ra)
    pass_on(GI_B1, GI_HB, "y", gi_sb, gi_hb, gi_rb)
    second_step(GO_A1, GO_B1, GO_A2, GO_B2, go_ra, go_rb, go_s2a, go_s2b, go_r2a, go_r2b)
    second_step(GI_A1, GI_B1, GI_A2, GI_B2, gi_ra, gi_rb, gi_s2a, gi_s2b, gi_r2a, gi_r2b)
    finish(GO_A2, GO_B2, go_r2a, go_r2b, o_out)
    finish(GI_A2, GI_B2, gi_r2a, gi_r2b, o_in)

    @pl.when(z == dp)
    def _():
        param_copy(PK_Z, 1, pk_y.at[0 : nz - 1], pk_y.at[0 : nz - 1]).wait_send()
        param_copy(AUX_Z, 1, aux_y.at[0 : nz - 1], aux_y.at[0 : nz - 1]).wait_send()

    for phase, axis, whole in sent:
        copy(phase, axis, peer(axis, 1), whole, whole).wait_send()


def store(a, b, c, out_a, out_b, out_c, sem):
    copies = [pltpu.make_async_copy(s, d, sem.at[i]) for i, (s, d) in enumerate(((a, out_a), (b, out_b), (c, out_c)))]
    for copy in copies:
        copy.start()
    for copy in copies:
        copy.wait()


def on_device(ny, nz, nd, tok, cot, win, wout, rate, freq, slog, dr, di, rr, ri, skip):
    rows, cols = tok.shape
    half = cols // 2
    states, c = rate.shape[1], skip.shape[1]
    own_ch, lanes, four = ny * c, ny * states, 4 * states
    V = pltpu.VMEM
    come = lambda n: 5 if n == 8 else n
    relayed = [
        V((nz, ny, c, half), BF16), V((ny, nz, c, half), BF16),
        V((3, ny, c, half), BF16), V((3, nz, c, half), BF16),
        V((come(nz), ny, c, half), BF16), V((come(ny), nz, c, half), BF16),
        V((ny, c, half), BF16), V((nz, c, half), BF16),
        V((ny, c, half), BF16), V((nz, c, half), BF16),
    ]
    vm = pl.BlockSpec(memory_space=pltpu.VMEM)
    drive = [jnp.swapaxes(a, 1, 2) for a in (dr, di)]
    args = (tok, cot, win, wout, rate, freq, *drive, rr, ri, skip)
    outs = pl.pallas_call(
        functools.partial(kernel, ny, nz, nd),
        out_shape=(
            jax.ShapeDtypeStruct((rows, cols), BF16),
            jax.ShapeDtypeStruct(win.shape, F32),
            jax.ShapeDtypeStruct(wout.shape, F32),
        ),
        in_specs=[pl.BlockSpec(memory_space=pltpu.SMEM)] + [pl.BlockSpec(memory_space=pltpu.HBM)] * len(args),
        out_specs=(vm, vm, vm),
        scratch_shapes=[
            *[V(a.shape, a.dtype) for a in args],
            V((c, four), BF16), V((8, lanes), F32),
            V((c, four), BF16), V((8, lanes), F32),
            V((ny, c, four), BF16), V((ny, 8, lanes), F32),
            V((nz, ny, c, half), BF16), V((ny, nz, c, half), BF16),
            V((nz, ny, c, half), BF16), V((ny, nz, c, half), BF16),
            V((nd, rows, own_ch), BF16), V((nd, rows, own_ch), BF16),
            V((nd, rows, own_ch), BF16), V((nd, rows, own_ch), BF16),
            V((2, lanes), F32), V((ny * nz, 2, lanes), F32),
            V((2, lanes), F32), V((ny * nz, 2, lanes), F32),
            V((ny * nz, 2, lanes), F32), V((ny * nz, 2, lanes), F32),
            V((rows, own_ch), BF16), V((nd, rows, own_ch), BF16),
            V((rows, own_ch), BF16), V((nd, rows, own_ch), BF16),
            *relayed, *relayed,
            *[V((own_ch, lanes), BF16)] * 4,
            *[V((rows, lanes), F32)] * 4,
            pltpu.SemaphoreType.DMA((PHASES,)),
            pltpu.SemaphoreType.DMA((PHASES,)),
            pltpu.SemaphoreType.DMA((2, 3)),
            pltpu.SemaphoreType.DMA((2, 8)),
            pltpu.SemaphoreType.DMA((nd,)),
            pltpu.SemaphoreType.DMA((len(args),)),
        ],
        compiler_params=pltpu.CompilerParams(
            collective_id=0, has_side_effects=True, vmem_limit_bytes=48 * 1024 * 1024
        ),
        name="mixer",
    )(slog, *[pltpu.with_memory_space_constraint(a, pltpu.HBM) for a in args])
    return pl.pallas_call(
        store,
        out_shape=tuple(jax.ShapeDtypeStruct(o.shape, o.dtype) for o in outs),
        in_specs=[vm] * 3,
        out_specs=(pl.BlockSpec(memory_space=pltpu.HBM),) * 3,
        scratch_shapes=[pltpu.SemaphoreType.DMA((3,))],
        compiler_params=pltpu.CompilerParams(vmem_limit_bytes=8 * 1024 * 1024),
        name="store",
    )(*outs)


def solution(mesh):
    nd = mesh.shape["dp"]
    nz = nd
    ny = mesh.shape["sp"] // nz
    return jax.shard_map(
        functools.partial(on_device, ny, nz, nd),
        mesh=mesh,
        in_specs=(
            P("sp", "dp"), P("sp", "dp"), P("sp", "dp"), P("sp", "dp"),
            P("sp", None), P("sp", None), P("sp"),
            P("sp", None, None), P("sp", None, None), P("sp", None, None), P("sp", None, None),
            P("sp", None),
        ),
        out_specs=(P("sp", "dp"), P("sp", "dp"), P("sp", "dp")),
        check_vma=False,
    )
```

```python
import functools
import math

import jax
import jax.numpy as jnp
from jax import lax
from jax.experimental import pallas as pl
from jax.experimental.pallas import tpu as pltpu
from jax.sharding import PartitionSpec as P

MESH = pl.DeviceIdType.MESH
F32 = jnp.float32
BF16 = jnp.bfloat16
HIGHEST = lax.Precision.HIGHEST

(
    IN_A1, IN_B1, IN_A2, IN_B2, OUT_A1, OUT_B1, OUT_A2, OUT_B2,
    PK_Z, AUX_Z, PK_Y, AUX_Y, DRIVE, BACK, FWD_Y, FWD_Z, BWD_Y, BWD_Z,
    GATED, MIX, GO_A1, GO_B1, GO_A2, GO_B2, GI_A1, GI_B1, GI_A2, GI_B2, GO_HA, GO_HB, GI_HA, GI_HB,
) = range(32)
PHASES = 32

NN = (((1,), (0,)), ((), ()))
NT = (((1,), (1,)), ((), ()))
TN = (((0,), (0,)), ((), ()))


def dot(a, b, dims=NN, precision=None):
    return lax.dot_general(a, b, dims, precision=precision, preferred_element_type=F32)


def cmul(a, b):
    return a[0] * b[0] - a[1] * b[1], a[0] * b[1] + a[1] * b[0]


def conj(a):
    return a[0], -a[1]


def square(a, times):
    for _ in range(times):
        a = (a[0] * a[0] - a[1] * a[1], 2.0 * a[0] * a[1])
    return a


def ring_order(n, far_first):
    ks = sorted(range(1, n), key=lambda k: (min(k, n - k), k))
    return ks[::-1] if far_first else ks


def slots(n):
    held = [0] + ring_order(n, False)
    return held, {k: i for i, k in enumerate(held)}


def slot_of(n, k):
    if n != 8:
        return k
    late = lax.div(k, 5)
    return (2 * k - 1) * (1 - late) + (16 - 2 * k) * late + 1 - lax.div(k + 7, 8)


def log2(n):
    return n.bit_length() - 1


def iota(shape, dim):
    return lax.broadcasted_iota(jnp.int32, shape, dim)


def scan_rows(pair, decay, reverse):
    re, im = pair
    rows, lanes = re.shape
    width = min(128, lanes)
    row = iota((rows, width), 0)
    outs = []
    for at in range(0, lanes, width):
        a, b = re[:, at : at + width], im[:, at : at + width]
        f = (decay[0][:, at : at + width], decay[1][:, at : at + width])
        for k in range(log2(rows)):
            step = 1 << k
            if reverse:
                turn, keep = rows - step, row < rows - step
            else:
                turn, keep = step, row >= step
            ra = jnp.where(keep, pltpu.roll(a, turn, 0), 0.0)
            rb = jnp.where(keep, pltpu.roll(b, turn, 0), 0.0)
            a, b = a + f[0] * ra - f[1] * rb, b + f[0] * rb + f[1] * ra
            f = square(f, 1)
        outs.append((a, b))
    return (
        jnp.concatenate([o[0] for o in outs], axis=1),
        jnp.concatenate([o[1] for o in outs], axis=1),
    )


def kernel(
    ny, nz, nd,
    slog, tok_h, cot_h, win_h, wout_h, rate_h, freq_h, dr_h, di_h, rr_h, ri_h, skip_h,
    o_tok, o_in, o_out,
    tok, cot, win, wout, rate, freq, dr, di, rr, ri, skip,
    pk_own, aux_own, pk_z, aux_z, pk_y, aux_y,
    wa_in, wb_in, wa_out, wb_out,
    d_send, d_recv, b_send, b_recv,
    f_own, f_recv, a_own, a_recv, w_re, w_im,
    gat_own, gat_all, mix_own, mix_all,
    go_sa, go_sb, go_ha, go_hb, go_ra, go_rb, go_s2a, go_s2b, go_r2a, go_r2b,
    gi_sa, gi_sb, gi_ha, gi_hb, gi_ra, gi_rb, gi_s2a, gi_s2b, gi_r2a, gi_r2b,
    bre, bim, cre, cim, u_re, u_im, v_re, v_im,
    ssem, rsem, in1_sem, in2_sem, mix_sem, load_sem,
):
    sp, dp = lax.axis_index("sp"), lax.axis_index("dp")
    z, y = lax.div(sp, ny), lax.rem(sp, ny)
    size = {"y": ny, "z": nz, "d": nd}
    here = {"y": y, "z": z, "d": dp}
    rows = tok.shape[0]
    states = rate.shape[1]
    per_group = skip.shape[1]
    own_ch = ny * per_group
    lanes = ny * states
    half = win.shape[1] // 2
    core = lax.rem(dp, 2)
    _, at_y = slots(ny)
    _, at_z = slots(nz)
    slot = {"y": lambda k: at_y[k % ny], "z": lambda k: at_z[k % nz]}

    def device(axis, j):
        if axis == "y":
            return (z * ny + j, dp)
        if axis == "z":
            return (j * ny + y, dp)
        return (sp, j)

    def peer(axis, k):
        return lax.rem(here[axis] + k, size[axis])

    def copy(phase, axis, j, src, dst, recv_sem=None):
        return pltpu.make_async_remote_copy(
            src_ref=src,
            dst_ref=dst,
            send_sem=ssem.at[phase],
            recv_sem=rsem.at[phase] if recv_sem is None else recv_sem,
            device_id=device(axis, j),
            device_id_type=MESH,
        )

    sent = []

    def send(phase, axis, src, dst, whole, sems=None):
        for k in ring_order(size[axis], True):
            copy(phase, axis, peer(axis, k), src(k), dst(k), None if sems is None else sems(k)).start()
        sent.append((phase, axis, whole))

    def arrive(phase, axis, whole):
        copy(phase, axis, peer(axis, 1), whole, whole).wait_recv()

    pairs = (
        (win_h, win), (wout_h, wout), (rate_h, rate), (freq_h, freq), (dr_h, dr), (di_h, di), (rr_h, rr),
        (ri_h, ri), (skip_h, skip), (tok_h, tok), (cot_h, cot),
    )
    loads = [pltpu.make_async_copy(a, b, load_sem.at[i]) for i, (a, b) in enumerate(pairs)]
    for load in loads:
        load.start()

    barrier = pltpu.get_barrier_semaphore()
    for axis in ("y", "z", "d"):
        for k in ring_order(size[axis], True):
            j = peer(axis, k)
            pl.semaphore_signal(barrier, inc=1, device_id=device(axis, j), device_id_type=MESH)

    pl.semaphore_wait(barrier, (ny - 1) + (nz - 1) + (nd - 1))

    for load in loads[:2]:
        load.wait()

    def parts(n):
        return ((0, 1), (1, 5), (5, 8)) if n == 8 else ((0, 1), (1, n))

    def part_of(n, at):
        return [a <= at < b for a, b in parts(n)].index(True)

    def spread(phase, axis, w, src, a, b, sems=None):
        for k in ring_order(size[axis], True):
            at = slot[axis](-k)
            dst = w.at[at, a] if b is None else w.at[at, a:b]
            copy(phase, axis, peer(axis, k), src, dst, None if sems is None else sems(at)).start()

    def gathered(phase, axis, w):
        arrive(phase, axis, w.at[1:])
        sent.append((phase, axis, w.at[1:]))

    left, right = win.at[:, 0:half], win.at[:, half:]
    send(
        IN_A1, "y", lambda k: left, lambda k: wa_in.at[0, at_y[-k % ny]], wa_in.at[0, 1:],
        lambda k: in1_sem.at[0, part_of(ny, at_y[-k % ny])],
    )
    send(
        IN_B1, "z", lambda k: right, lambda k: wb_in.at[0, at_z[-k % nz]], wb_in.at[0, 1:],
        lambda k: in1_sem.at[1, part_of(nz, at_z[-k % nz])],
    )
    spread(IN_A2, "z", wa_in, left, 0, None, lambda at: in2_sem.at[0, at])
    spread(IN_B2, "y", wb_in, right, 0, None, lambda at: in2_sem.at[1, 0])
    wa_in[0, 0] = win[:, 0:half]
    wb_in[0, 0] = win[:, half:]
    wa_out[0, 0] = wout[:, 0:half]
    wb_out[0, 0] = wout[:, half:]
    for load in loads[2:9]:
        load.wait()

    tile_s = (iota((states, lanes), 0) == lax.rem(iota((states, lanes), 1), states)).astype(F32)
    wide = lambda ref: dot(jnp.broadcast_to(ref[...], (8, states)), tile_s, precision=HIGHEST)
    rate_w, freq_w = wide(rate), wide(freq)
    step = jnp.exp(jnp.full((8, lanes), slog[0], F32))
    magnitude = jnp.exp(-rate_w * step)
    angle = freq_w * step
    dec_re, dec_im = magnitude * jnp.cos(angle), magnitude * jnp.sin(angle)
    modulus = rate_w * rate_w + freq_w * freq_w
    hold_re = (-rate_w * (dec_re - 1.0) + freq_w * dec_im) / modulus
    hold_im = (-freq_w * (dec_re - 1.0) - rate_w * dec_im) / modulus
    tile_c = (
        iota((per_group, lanes), 0) == lax.rem(iota((per_group, lanes), 1), per_group)
    ).astype(F32)
    skip_w = dot(jnp.broadcast_to(skip[...], (8, per_group)), tile_c, precision=HIGHEST)
    row8 = iota((8, lanes), 0)
    aux_own[...] = jnp.where(row8 == 0, dec_re, jnp.where(row8 == 1, dec_im, skip_w))
    four = 4 * states
    p_row, p_lane = iota((states, four), 0), iota((states, four), 1)
    hr, hi = hold_re[0:1, 0:states], hold_im[0:1, 0:states]
    hr = jnp.concatenate([hr] * 4, axis=1) if four > lanes else hold_re[0:1, 0:four]
    hi = jnp.concatenate([hi] * 4, axis=1) if four > lanes else hold_im[0:1, 0:four]
    first, second = p_lane == p_row, p_lane == p_row + states
    sel_r = jnp.where(first, hr, 0.0) + jnp.where(second, hi, 0.0)
    sel_i = jnp.where(first, -hi, 0.0) + jnp.where(second, hr, 0.0)
    sel_c = (p_lane == p_row + 2 * states).astype(F32)
    sel_d = (p_lane == p_row + 3 * states).astype(F32)
    pk_own[...] = (
        dot(dr[0], sel_r, NN, HIGHEST)
        + dot(di[0], sel_i, NN, HIGHEST)
        + dot(rr[0], sel_c, NN, HIGHEST)
        + dot(ri[0], sel_d, NN, HIGHEST)
    ).astype(BF16)

    def param_copy(phase, k, src, dst):
        return copy(phase, "z", peer("z", k), src, dst)

    @pl.when(z == dp)
    def _():
        for k in ring_order(nz, True):
            param_copy(PK_Z, k, pk_own, pk_z).start()
            param_copy(AUX_Z, k, aux_own, aux_z).start()
        pk_z[...] = pk_own[...]
        aux_z[...] = aux_own[...]

    def forward(part):
        if part < len(parts(ny)):
            a, b = parts(ny)[part]
            own = wa_in.at[0, a:b]
            copy(IN_A1, "y", peer("y", 1), own, own, in1_sem.at[0, part]).wait_recv()
            spread(IN_A2, "z", wa_in, own, a, b, lambda at: in2_sem.at[0, at])
        if part < len(parts(nz)):
            a, b = parts(nz)[part]
            own = wb_in.at[0, a:b]
            copy(IN_B1, "z", peer("z", 1), own, own, in1_sem.at[1, part]).wait_recv()
            spread(IN_B2, "y", wb_in, own, a, b, lambda at: in2_sem.at[1, part])

    forward(1)
    send(OUT_A1, "y", lambda k: wout.at[:, 0:half], lambda k: wa_out.at[0, at_y[-k % ny]], wa_out.at[0, 1:])
    send(OUT_B1, "z", lambda k: wout.at[:, half:], lambda k: wb_out.at[0, at_z[-k % nz]], wb_out.at[0, 1:])
    if max(ny, nz) > 2:
        forward(2)

    @pl.when(z != dp)
    def _():
        param_copy(PK_Z, 1, pk_z, pk_z).wait_recv()
        param_copy(AUX_Z, 1, aux_z, aux_z).wait_recv()

    send(PK_Y, "y", lambda k: pk_z, lambda k: pk_y.at[y], pk_y.at[1:])
    send(AUX_Y, "y", lambda k: aux_z, lambda k: aux_y.at[y], aux_y.at[1:])
    pk_y[y] = pk_z[...]
    aux_y[y] = aux_z[...]


    def weights_of(wa, wb, b):
        return weights_at(wa, wb, slot_of(nz, lax.rem(b - z + nz, nz)))

    def weights_at(wa, wb, at):
        place = [slot_of(ny, lax.rem(g - y + ny, ny)) for g in range(ny)]
        left = jnp.concatenate([wa[at, i] for i in place], axis=0)
        right = jnp.concatenate([wb[i, at] for i in place], axis=0)
        return jnp.concatenate([left, right], axis=1)

    def project(phase, act, wa, wb, out, recv):
        for k in ring_order(nd, True):
            j = peer("d", k)
            out[j] = dot(act[...], weights_of(wa, wb, j), NT).astype(BF16)
            copy(phase, "d", j, out.at[j], recv.at[dp]).start()
        sent.append((phase, "d", recv.at[0 : nd - 1]))
        recv[dp] = dot(act[...], weights_of(wa, wb, dp), NT).astype(BF16)

    for load in loads[9:]:
        load.wait()
    for part, (a, e) in enumerate(parts(nz)):
        got = wb_in.at[1:, a:e]
        copy(IN_B2, "y", peer("y", 1), got, got, in2_sem.at[1, part]).wait_recv()
        for at in range(max(a, 1), e):
            copy(IN_A2, "z", peer("z", 1), wa_in.at[at], wa_in.at[at], in2_sem.at[0, at]).wait_recv()
        targets = [peer("z", slots(nz)[0][at]) for at in range(a, e)]
        for at, b in zip(range(a, e), targets):
            d_send[b] = dot(tok[...], weights_at(wa_in, wb_in, at), NT).astype(BF16)

            @pl.when(b != dp)
            def _():
                copy(DRIVE, "d", b, d_send.at[b], d_recv.at[dp]).start()

            @pl.when(b == dp)
            def _():
                d_recv[dp] = d_send[dp]

        if part == 1:
            arrive(OUT_A1, "y", wa_out.at[0, 1:])
            spread(OUT_A2, "z", wa_out, wa_out.at[0, 0:ny], 0, ny)
            arrive(OUT_B1, "z", wb_out.at[0, 1:])
            spread(OUT_B2, "y", wb_out, wb_out.at[0, 0:nz], 0, nz)

    sent.append((IN_A2, "z", wa_in.at[1:]))
    sent.append((IN_B2, "y", wb_in.at[1:]))
    sent.append((DRIVE, "d", d_recv.at[0 : nd - 1]))

    arrive(PK_Y, "y", pk_y.at[0 : ny - 1])
    arrive(AUX_Y, "y", aux_y.at[0 : ny - 1])
    packed = pk_y[...].reshape(own_ch, four)
    diag = lax.div(iota((own_ch, lanes), 0), per_group) == lax.div(iota((own_ch, lanes), 1), states)
    s_row, s_lane = iota((four, lanes), 0), lax.rem(iota((four, lanes), 1), states)
    for at, ref in enumerate((bre, bim, cre, cim)):
        spread = (s_row == s_lane + at * states).astype(F32).astype(BF16)
        ref[...] = jnp.where(diag, dot(packed, spread), 0.0).astype(BF16)
    group_of_lane = lax.div(iota((1, lanes), 1), states)
    group_of_ch = lax.div(iota((1, own_ch), 1), per_group)
    dec = (jnp.zeros((1, lanes), F32), jnp.zeros((1, lanes), F32))
    gain = jnp.zeros((1, own_ch), F32)
    for g in range(ny):
        dec = (
            jnp.where(group_of_lane == g, aux_y[g, 0:1, :], dec[0]),
            jnp.where(group_of_lane == g, aux_y[g, 1:2, :], dec[1]),
        )
        gain = jnp.where(group_of_ch == g, aux_y[g, 2:3, 0:own_ch], gain)
    row = iota((rows, lanes), 0)
    up = (jnp.ones((rows, lanes), F32), jnp.zeros((rows, lanes), F32))
    down = up
    factor = dec
    for k in range(log2(rows)):
        bit = lax.rem(lax.div(row, 1 << k), 2) == 1
        more = cmul(up, factor)
        up = (jnp.where(bit, more[0], up[0]), jnp.where(bit, more[1], up[1]))
        more = cmul(down, factor)
        down = (jnp.where(bit, down[0], more[0]), jnp.where(bit, down[1], more[1]))
        factor = square(factor, 1)
    u_re[...], u_im[...] = up
    v_re[...], v_im[...] = down
    dec_chunk = factor

    def total(recv):
        s = recv[0].astype(F32)
        for b in range(1, nd):
            s = s + recv[b].astype(F32)
        return s.astype(BF16)

    arrive(DRIVE, "d", d_recv.at[0 : nd - 1])
    x = total(d_recv)

    chunks = ny * nz

    def to_all(phase, own, recv, reverse):
        far = lambda k, n: min(k, n - k)
        offsets = [(a, b) for a in range(nz) for b in range(ny) if a or b]
        for a, b in sorted(offsets, key=lambda o: -far(o[0], nz) - far(o[1], ny)):
            j = peer("z", a) * ny + peer("y", b)
            ahead = sp - j if reverse else j - sp
            pltpu.make_async_remote_copy(
                src_ref=own,
                dst_ref=recv.at[lax.rem(ahead - 1 + 2 * chunks, chunks)],
                send_sem=ssem.at[phase],
                recv_sem=rsem.at[phase],
                device_id=(j, dp),
                device_id_type=MESH,
            ).start()
        sent.append((phase, "y", recv.at[1:]))

    def entering(recv, reverse):
        held = iota((chunks, 2, lanes), 0) < (chunks - 1 - sp if reverse else sp)
        state = jnp.where(held, recv[...].astype(F32), 0.0)
        by_re = jnp.sum(state * w_re[...], axis=0)
        by_im = jnp.sum(state * w_im[...], axis=0)
        if reverse:
            by_im = -by_im
        return by_re[0:1] - by_im[1:2], by_re[1:2] + by_im[0:1]

    def summed(pair, table_re, table_im, sign):
        tr, ti = table_re[...], sign * table_im[...]
        re, im = cmul(pair, (tr, ti))
        return jnp.sum(re, axis=0, keepdims=True), jnp.sum(im, axis=0, keepdims=True)

    def put(ref, pair):
        ref[...] = jnp.concatenate(pair, axis=0).astype(ref.dtype)

    push = (dot(x, bre[...]), dot(x, bim[...]))
    final = summed(push, v_re, v_im, 1.0)
    put(f_own, final)
    to_all(FWD_Y, f_own, f_recv, False)
    local = scan_rows(push, dec, False)
    gathered(OUT_A2, "z", wa_out)
    gathered(OUT_B2, "y", wb_out)
    project(BACK, cot, wa_out, wb_out, b_send, b_recv)

    row = iota((chunks, lanes), 0)
    power, factor = (jnp.ones((chunks, lanes), F32), jnp.zeros((chunks, lanes), F32)), dec_chunk
    for k in range(log2(chunks)):
        bit = lax.rem(lax.div(row, 1 << k), 2) == 1
        more = cmul(power, factor)
        power = (jnp.where(bit, more[0], power[0]), jnp.where(bit, more[1], power[1]))
        factor = square(factor, 1)
    w_re[...] = jnp.broadcast_to(power[0][:, None, :], (chunks, 2, lanes))
    w_im[...] = jnp.broadcast_to(power[1][:, None, :], (chunks, 2, lanes))
    arrive(FWD_Y, "y", f_recv.at[1:])
    start = cmul(dec, entering(f_recv, False))
    add = cmul((u_re[...], u_im[...]), start)
    state_re, state_im = (local[0] + add[0]).astype(BF16), (local[1] + add[1]).astype(BF16)
    mixed = dot(state_re, cre[...], NT) - dot(state_im, cim[...], NT) + gain * x.astype(F32)
    c0 = math.sqrt(2.0 / math.pi)
    sq = mixed * mixed
    th = jnp.tanh(c0 * mixed * (1.0 + 0.044715 * sq))
    half_up = 0.5 * (1.0 + th)
    gated = (mixed * half_up).astype(BF16)
    slope = half_up + 0.5 * mixed * (1.0 - th * th) * (c0 * (1.0 + 3.0 * 0.044715 * sq))
    arrive(BACK, "d", b_recv.at[0 : nd - 1])
    inner = slope * total(b_recv).astype(F32)
    inner_b = inner.astype(BF16)
    pulled = (dot(inner_b, cre[...]), -dot(inner_b, cim[...]))
    opening = summed(pulled, u_re, u_im, -1.0)
    put(a_own, opening)
    to_all(BWD_Y, a_own, a_recv, True)
    gat_own[...] = gated
    send(GATED, "d", lambda k: gat_own, lambda k: gat_all.at[dp], gat_all.at[0 : nd - 1])
    gat_all[dp] = gated
    back_dec = conj(dec)
    local = scan_rows(pulled, back_dec, True)
    def block_of_grad(b, cols, act, sa, sb):
        part = dot(cols[b], act[...], TN).astype(BF16)
        sa[b] = part[:, 0:half].reshape(ny, per_group, half)
        sb[:, b] = part[:, half:].reshape(ny, per_group, half)

    def hand_on(phase, phase_h, axis, s, h, r):
        if size[axis] != 8:
            for k in ring_order(size[axis], True):
                copy(phase, axis, peer(axis, k), s.at[peer(axis, k)], r.at[slot[axis](-k)]).start()
            sent.append((phase, axis, r.at[1:]))
        else:
            copy(phase_h, axis, peer(axis, 2 + 4 * core), s.at[peer(axis, 4)], h.at[2]).start()
            copy(phase_h, axis, peer(axis, 1), s.at[peer(axis, 3)], h.at[0]).start()
            copy(phase_h, axis, peer(axis, 7), s.at[peer(axis, 5)], h.at[1]).start()
            copy(phase, axis, peer(axis, 1), s.at[peer(axis, 1)], r.at[1]).start()
            copy(phase, axis, peer(axis, 7), s.at[peer(axis, 7)], r.at[2]).start()
        r[0] = s[here[axis]]

    def add_to(s, j, part):
        s[j] = (s[j].astype(F32) + part.astype(F32)).astype(BF16)

    def pass_on(phase, phase_h, axis, s, h, r):
        if size[axis] == 8:
            arrive(phase_h, axis, h)
            add_to(s, peer(axis, 2), h[0])
            add_to(s, peer(axis, 6), h[1])
            add_to(s, peer(axis, 2 + 4 * core), h[2])
            copy(phase, axis, peer(axis, 2), s.at[peer(axis, 2)], r.at[3]).start()
            copy(phase, axis, peer(axis, 6), s.at[peer(axis, 6)], r.at[4]).start()
            sent.append((phase_h, axis, h))
            sent.append((phase, axis, r.at[1:]))

    def reduced(recv, n):
        s = recv[0].astype(F32)
        for j in range(1, n):
            s = s + recv[j].astype(F32)
        return s

    def second_step(phase_a1, phase_b1, phase_a2, phase_b2, ra, rb, s2a, s2b, r2a, r2b):
        arrive(phase_a1, "z", ra.at[1:])
        s2a[...] = reduced(ra, ra.shape[0]).astype(BF16)
        send(phase_a2, "y", lambda k: s2a.at[peer("y", k)], lambda k: r2a.at[at_y[-k % ny]], r2a.at[1:])
        r2a[0] = s2a[y]
        arrive(phase_b1, "y", rb.at[1:])
        s2b[...] = reduced(rb, rb.shape[0]).astype(BF16)
        send(phase_b2, "z", lambda k: s2b.at[peer("z", k)], lambda k: r2b.at[at_z[-k % nz]], r2b.at[1:])
        r2b[0] = s2b[z]

    scale = (rows * ny * nz) ** -0.5

    def finish(phase_a2, phase_b2, r2a, r2b, out):
        arrive(phase_a2, "y", r2a.at[0 : ny - 1])
        arrive(phase_b2, "z", r2b.at[0 : nz - 1])
        out[:, 0:half] = reduced(r2a, ny) * scale
        out[:, half:] = reduced(r2b, nz) * scale

    arrive(GATED, "d", gat_all.at[0 : nd - 1])
    for b in range(nd):
        block_of_grad(b, gat_all, cot, go_sa, go_sb)
    hand_on(GO_A1, GO_HA, "z", go_sa, go_ha, go_ra)
    hand_on(GO_B1, GO_HB, "y", go_sb, go_hb, go_rb)

    arrive(BWD_Y, "y", a_recv.at[1:])
    start = cmul(back_dec, entering(a_recv, True))
    add = cmul((v_re[...], -v_im[...]), start)
    adj_re, adj_im = (local[0] + add[0]).astype(BF16), (local[1] + add[1]).astype(BF16)
    mix = (dot(adj_re, bre[...], NT) + dot(adj_im, bim[...], NT) + gain * inner).astype(BF16)
    mix_own[...] = mix
    send(MIX, "d", lambda k: mix_own, lambda k: mix_all.at[dp], mix_all.at[0 : nd - 1], lambda k: mix_sem.at[k])
    mix_all[dp] = mix

    block_of_grad(dp, mix_all, tok, gi_sa, gi_sb)
    order = ring_order(nd, False)
    for batch in (order[0:1], order[1:2], order[2:]):
        for k in batch:
            j = peer("d", nd - k)
            copy(MIX, "d", j, mix_own, mix_all.at[j], mix_sem.at[k]).wait_recv()
        for k in batch:
            block_of_grad(peer("d", nd - k), mix_all, tok, gi_sa, gi_sb)
        if batch == order[1:2]:
            pass_on(GO_A1, GO_HA, "z", go_sa, go_ha, go_ra)
            pass_on(GO_B1, GO_HB, "y", go_sb, go_hb, go_rb)
    hand_on(GI_A1, GI_HA, "z", gi_sa, gi_ha, gi_ra)
    hand_on(GI_B1, GI_HB, "y", gi_sb, gi_hb, gi_rb)
    grad = dot(mix_all[0], weights_of(wa_in, wb_in, 0))
    for b in range(1, nd):
        grad = grad + dot(mix_all[b], weights_of(wa_in, wb_in, b))
    o_tok[...] = grad.astype(BF16)
    pass_on(GI_A1, GI_HA, "z", gi_sa, gi_ha, gi_ra)
    pass_on(GI_B1, GI_HB, "y", gi_sb, gi_hb, gi_rb)
    second_step(GO_A1, GO_B1, GO_A2, GO_B2, go_ra, go_rb, go_s2a, go_s2b, go_r2a, go_r2b)
    second_step(GI_A1, GI_B1, GI_A2, GI_B2, gi_ra, gi_rb, gi_s2a, gi_s2b, gi_r2a, gi_r2b)
    finish(GO_A2, GO_B2, go_r2a, go_r2b, o_out)
    finish(GI_A2, GI_B2, gi_r2a, gi_r2b, o_in)

    @pl.when(z == dp)
    def _():
        param_copy(PK_Z, 1, pk_y.at[0 : nz - 1], pk_y.at[0 : nz - 1]).wait_send()
        param_copy(AUX_Z, 1, aux_y.at[0 : nz - 1], aux_y.at[0 : nz - 1]).wait_send()

    for phase, axis, whole in sent:
        copy(phase, axis, peer(axis, 1), whole, whole).wait_send()


def store(a, b, c, out_a, out_b, out_c, sem):
    copies = [pltpu.make_async_copy(s, d, sem.at[i]) for i, (s, d) in enumerate(((a, out_a), (b, out_b), (c, out_c)))]
    for copy in copies:
        copy.start()
    for copy in copies:
        copy.wait()


def on_device(ny, nz, nd, tok, cot, win, wout, rate, freq, slog, dr, di, rr, ri, skip):
    rows, cols = tok.shape
    half = cols // 2
    states, c = rate.shape[1], skip.shape[1]
    own_ch, lanes, four = ny * c, ny * states, 4 * states
    V = pltpu.VMEM
    come = lambda n: 5 if n == 8 else n
    relayed = [
        V((nz, ny, c, half), BF16), V((ny, nz, c, half), BF16),
        V((3, ny, c, half), BF16), V((3, nz, c, half), BF16),
        V((come(nz), ny, c, half), BF16), V((come(ny), nz, c, half), BF16),
        V((ny, c, half), BF16), V((nz, c, half), BF16),
        V((ny, c, half), BF16), V((nz, c, half), BF16),
    ]
    vm = pl.BlockSpec(memory_space=pltpu.VMEM)
    drive = [jnp.swapaxes(a, 1, 2) for a in (dr, di)]
    args = (tok, cot, win, wout, rate, freq, *drive, rr, ri, skip)
    outs = pl.pallas_call(
        functools.partial(kernel, ny, nz, nd),
        out_shape=(
            jax.ShapeDtypeStruct((rows, cols), BF16),
            jax.ShapeDtypeStruct(win.shape, F32),
            jax.ShapeDtypeStruct(wout.shape, F32),
        ),
        in_specs=[pl.BlockSpec(memory_space=pltpu.SMEM)] + [pl.BlockSpec(memory_space=pltpu.HBM)] * len(args),
        out_specs=(vm, vm, vm),
        scratch_shapes=[
            *[V(a.shape, a.dtype) for a in args],
            V((c, four), BF16), V((8, lanes), F32),
            V((c, four), BF16), V((8, lanes), F32),
            V((ny, c, four), BF16), V((ny, 8, lanes), F32),
            V((nz, ny, c, half), BF16), V((ny, nz, c, half), BF16),
            V((nz, ny, c, half), BF16), V((ny, nz, c, half), BF16),
            V((nd, rows, own_ch), BF16), V((nd, rows, own_ch), BF16),
            V((nd, rows, own_ch), BF16), V((nd, rows, own_ch), BF16),
            V((2, lanes), BF16), V((ny * nz, 2, lanes), BF16),
            V((2, lanes), BF16), V((ny * nz, 2, lanes), BF16),
            V((ny * nz, 2, lanes), F32), V((ny * nz, 2, lanes), F32),
            V((rows, own_ch), BF16), V((nd, rows, own_ch), BF16),
            V((rows, own_ch), BF16), V((nd, rows, own_ch), BF16),
            *relayed, *relayed,
            *[V((own_ch, lanes), BF16)] * 4,
            *[V((rows, lanes), F32)] * 4,
            pltpu.SemaphoreType.DMA((PHASES,)),
            pltpu.SemaphoreType.DMA((PHASES,)),
            pltpu.SemaphoreType.DMA((2, 3)),
            pltpu.SemaphoreType.DMA((2, 8)),
            pltpu.SemaphoreType.DMA((nd,)),
            pltpu.SemaphoreType.DMA((len(args),)),
        ],
        compiler_params=pltpu.CompilerParams(
            collective_id=0, has_side_effects=True, vmem_limit_bytes=48 * 1024 * 1024
        ),
        name="mixer",
    )(slog, *[pltpu.with_memory_space_constraint(a, pltpu.HBM) for a in args])
    return pl.pallas_call(
        store,
        out_shape=tuple(jax.ShapeDtypeStruct(o.shape, o.dtype) for o in outs),
        in_specs=[vm] * 3,
        out_specs=(pl.BlockSpec(memory_space=pltpu.HBM),) * 3,
        scratch_shapes=[pltpu.SemaphoreType.DMA((3,))],
        compiler_params=pltpu.CompilerParams(vmem_limit_bytes=8 * 1024 * 1024),
        name="store",
    )(*outs)


def solution(mesh):
    nd = mesh.shape["dp"]
    nz = nd
    ny = mesh.shape["sp"] // nz
    return jax.shard_map(
        functools.partial(on_device, ny, nz, nd),
        mesh=mesh,
        in_specs=(
            P("sp", "dp"), P("sp", "dp"), P("sp", "dp"), P("sp", "dp"),
            P("sp", None), P("sp", None), P("sp"),
            P("sp", None, None), P("sp", None, None), P("sp", None, None), P("sp", None, None),
            P("sp", None),
        ),
        out_specs=(P("sp", "dp"), P("sp", "dp"), P("sp", "dp")),
        check_vma=False,
    )
```

```python
import functools
import math

import jax
import jax.numpy as jnp
from jax import lax
from jax.experimental import pallas as pl
from jax.experimental.pallas import tpu as pltpu
from jax.sharding import PartitionSpec as P

MESH = pl.DeviceIdType.MESH
F32 = jnp.float32
BF16 = jnp.bfloat16
HIGHEST = lax.Precision.HIGHEST

(
    IN_A1, IN_B1, IN_A2, IN_B2, OUT_A1, OUT_B1, OUT_A2, OUT_B2,
    PK_Z, AUX_Z, PK_Y, AUX_Y, DRIVE, BACK, FWD_Y, FWD_Z, BWD_Y, BWD_Z,
    GATED, MIX, GO_A1, GO_B1, GO_A2, GO_B2, GI_A1, GI_B1, GI_A2, GI_B2, GO_HA, GO_HB, GI_HA, GI_HB,
) = range(32)
PHASES = 32

NN = (((1,), (0,)), ((), ()))
NT = (((1,), (1,)), ((), ()))
TN = (((0,), (0,)), ((), ()))


def dot(a, b, dims=NN, precision=None):
    return lax.dot_general(a, b, dims, precision=precision, preferred_element_type=F32)


def cmul(a, b):
    return a[0] * b[0] - a[1] * b[1], a[0] * b[1] + a[1] * b[0]


def conj(a):
    return a[0], -a[1]


def square(a, times):
    for _ in range(times):
        a = (a[0] * a[0] - a[1] * a[1], 2.0 * a[0] * a[1])
    return a


def ring_order(n, far_first):
    ks = sorted(range(1, n), key=lambda k: (min(k, n - k), k))
    return ks[::-1] if far_first else ks


def slots(n):
    held = [0] + ring_order(n, False)
    return held, {k: i for i, k in enumerate(held)}


def slot_of(n, k):
    if n != 8:
        return k
    late = lax.div(k, 5)
    return (2 * k - 1) * (1 - late) + (16 - 2 * k) * late + 1 - lax.div(k + 7, 8)


def log2(n):
    return n.bit_length() - 1


def iota(shape, dim):
    return lax.broadcasted_iota(jnp.int32, shape, dim)


def scan_rows(pair, decay, reverse):
    re, im = pair
    rows, lanes = re.shape
    width = min(128, lanes)
    row = iota((rows, width), 0)
    outs = []
    for at in range(0, lanes, width):
        a, b = re[:, at : at + width], im[:, at : at + width]
        f = (decay[0][:, at : at + width], decay[1][:, at : at + width])
        for k in range(log2(rows)):
            step = 1 << k
            if reverse:
                turn, keep = rows - step, row < rows - step
            else:
                turn, keep = step, row >= step
            ra = jnp.where(keep, pltpu.roll(a, turn, 0), 0.0)
            rb = jnp.where(keep, pltpu.roll(b, turn, 0), 0.0)
            a, b = a + f[0] * ra - f[1] * rb, b + f[0] * rb + f[1] * ra
            f = square(f, 1)
        outs.append((a, b))
    return (
        jnp.concatenate([o[0] for o in outs], axis=1),
        jnp.concatenate([o[1] for o in outs], axis=1),
    )


def kernel(
    ny, nz, nd,
    slog, tok_h, cot_h, win_h, wout_h, rate_h, freq_h, dr_h, di_h, rr_h, ri_h, skip_h,
    o_tok, o_in, o_out,
    tok, cot, win, wout, rate, freq, dr, di, rr, ri, skip,
    pk_own, aux_own, pk_z, aux_z, pk_y, aux_y,
    wa_in, wb_in, wa_out, wb_out,
    d_send, d_recv, b_send, b_recv,
    f_own, f_recv, a_own, a_recv, w_re, w_im,
    gat_own, gat_all, mix_own, mix_all,
    go_sa, go_sb, go_ha, go_hb, go_ra, go_rb, go_s2a, go_s2b, go_r2a, go_r2b,
    gi_sa, gi_sb, gi_ha, gi_hb, gi_ra, gi_rb, gi_s2a, gi_s2b, gi_r2a, gi_r2b,
    bre, bim, cre, cim, u_re, u_im, v_re, v_im,
    ssem, rsem, in1_sem, in2_sem, mix_sem, load_sem,
):
    sp, dp = lax.axis_index("sp"), lax.axis_index("dp")
    z, y = lax.div(sp, ny), lax.rem(sp, ny)
    size = {"y": ny, "z": nz, "d": nd}
    here = {"y": y, "z": z, "d": dp}
    rows = tok.shape[0]
    states = rate.shape[1]
    per_group = skip.shape[1]
    own_ch = ny * per_group
    lanes = ny * states
    half = win.shape[1] // 2
    core = lax.rem(dp, 2)
    _, at_y = slots(ny)
    _, at_z = slots(nz)
    slot = {"y": lambda k: at_y[k % ny], "z": lambda k: at_z[k % nz]}

    def device(axis, j):
        if axis == "y":
            return (z * ny + j, dp)
        if axis == "z":
            return (j * ny + y, dp)
        return (sp, j)

    def peer(axis, k):
        return lax.rem(here[axis] + k, size[axis])

    def copy(phase, axis, j, src, dst, recv_sem=None):
        return pltpu.make_async_remote_copy(
            src_ref=src,
            dst_ref=dst,
            send_sem=ssem.at[phase],
            recv_sem=rsem.at[phase] if recv_sem is None else recv_sem,
            device_id=device(axis, j),
            device_id_type=MESH,
        )

    sent = []

    def send(phase, axis, src, dst, whole, sems=None):
        for k in ring_order(size[axis], True):
            copy(phase, axis, peer(axis, k), src(k), dst(k), None if sems is None else sems(k)).start()
        sent.append((phase, axis, whole))

    def arrive(phase, axis, whole):
        copy(phase, axis, peer(axis, 1), whole, whole).wait_recv()

    pairs = (
        (win_h, win), (wout_h, wout), (rate_h, rate), (freq_h, freq), (dr_h, dr), (di_h, di), (rr_h, rr),
        (ri_h, ri), (skip_h, skip), (tok_h, tok), (cot_h, cot),
    )
    loads = [pltpu.make_async_copy(a, b, load_sem.at[i]) for i, (a, b) in enumerate(pairs)]
    for load in loads:
        load.start()

    barrier = pltpu.get_barrier_semaphore()
    for axis in ("y", "z", "d"):
        for k in ring_order(size[axis], True):
            j = peer(axis, k)
            pl.semaphore_signal(barrier, inc=1, device_id=device(axis, j), device_id_type=MESH)

    pl.semaphore_wait(barrier, (ny - 1) + (nz - 1) + (nd - 1))

    for load in loads[:2]:
        load.wait()

    def parts(n):
        return ((0, 1), (1, 5), (5, 8)) if n == 8 else ((0, 1), (1, n))

    def part_of(n, at):
        return [a <= at < b for a, b in parts(n)].index(True)

    def spread(phase, axis, w, src, a, b, sems=None):
        for k in ring_order(size[axis], True):
            at = slot[axis](-k)
            dst = w.at[at, a] if b is None else w.at[at, a:b]
            copy(phase, axis, peer(axis, k), src, dst, None if sems is None else sems(at)).start()

    def gathered(phase, axis, w):
        arrive(phase, axis, w.at[1:])
        sent.append((phase, axis, w.at[1:]))

    left, right = win.at[:, 0:half], win.at[:, half:]
    send(
        IN_A1, "y", lambda k: left, lambda k: wa_in.at[0, at_y[-k % ny]], wa_in.at[0, 1:],
        lambda k: in1_sem.at[0, part_of(ny, at_y[-k % ny])],
    )
    send(
        IN_B1, "z", lambda k: right, lambda k: wb_in.at[0, at_z[-k % nz]], wb_in.at[0, 1:],
        lambda k: in1_sem.at[1, part_of(nz, at_z[-k % nz])],
    )
    spread(IN_A2, "z", wa_in, left, 0, None, lambda at: in2_sem.at[0, at])
    spread(IN_B2, "y", wb_in, right, 0, None, lambda at: in2_sem.at[1, 0])
    wa_in[0, 0] = win[:, 0:half]
    wb_in[0, 0] = win[:, half:]
    wa_out[0, 0] = wout[:, 0:half]
    wb_out[0, 0] = wout[:, half:]
    for load in loads[2:9]:
        load.wait()

    tile_s = (iota((states, lanes), 0) == lax.rem(iota((states, lanes), 1), states)).astype(F32)
    wide = lambda ref: dot(jnp.broadcast_to(ref[...], (8, states)), tile_s, precision=HIGHEST)
    rate_w, freq_w = wide(rate), wide(freq)
    step = jnp.exp(jnp.full((8, lanes), slog[0], F32))
    magnitude = jnp.exp(-rate_w * step)
    angle = freq_w * step
    dec_re, dec_im = magnitude * jnp.cos(angle), magnitude * jnp.sin(angle)
    modulus = rate_w * rate_w + freq_w * freq_w
    hold_re = (-rate_w * (dec_re - 1.0) + freq_w * dec_im) / modulus
    hold_im = (-freq_w * (dec_re - 1.0) - rate_w * dec_im) / modulus
    tile_c = (
        iota((per_group, lanes), 0) == lax.rem(iota((per_group, lanes), 1), per_group)
    ).astype(F32)
    skip_w = dot(jnp.broadcast_to(skip[...], (8, per_group)), tile_c, precision=HIGHEST)
    row8 = iota((8, lanes), 0)
    aux_own[...] = jnp.where(row8 == 0, dec_re, jnp.where(row8 == 1, dec_im, skip_w))
    four = 4 * states
    p_row, p_lane = iota((states, four), 0), iota((states, four), 1)
    hr, hi = hold_re[0:1, 0:states], hold_im[0:1, 0:states]
    hr = jnp.concatenate([hr] * 4, axis=1) if four > lanes else hold_re[0:1, 0:four]
    hi = jnp.concatenate([hi] * 4, axis=1) if four > lanes else hold_im[0:1, 0:four]
    first, second = p_lane == p_row, p_lane == p_row + states
    sel_r = jnp.where(first, hr, 0.0) + jnp.where(second, hi, 0.0)
    sel_i = jnp.where(first, -hi, 0.0) + jnp.where(second, hr, 0.0)
    sel_c = (p_lane == p_row + 2 * states).astype(F32)
    sel_d = (p_lane == p_row + 3 * states).astype(F32)
    pk_own[...] = (
        dot(dr[0], sel_r, NN, HIGHEST)
        + dot(di[0], sel_i, NN, HIGHEST)
        + dot(rr[0], sel_c, NN, HIGHEST)
        + dot(ri[0], sel_d, NN, HIGHEST)
    ).astype(BF16)

    def param_copy(phase, k, src, dst):
        return copy(phase, "z", peer("z", k), src, dst)

    @pl.when(z == dp)
    def _():
        for k in ring_order(nz, True):
            param_copy(PK_Z, k, pk_own, pk_z).start()
            param_copy(AUX_Z, k, aux_own, aux_z).start()
        pk_z[...] = pk_own[...]
        aux_z[...] = aux_own[...]

    def forward(part):
        if part < len(parts(ny)):
            a, b = parts(ny)[part]
            own = wa_in.at[0, a:b]
            copy(IN_A1, "y", peer("y", 1), own, own, in1_sem.at[0, part]).wait_recv()
            spread(IN_A2, "z", wa_in, own, a, b, lambda at: in2_sem.at[0, at])
        if part < len(parts(nz)):
            a, b = parts(nz)[part]
            own = wb_in.at[0, a:b]
            copy(IN_B1, "z", peer("z", 1), own, own, in1_sem.at[1, part]).wait_recv()
            spread(IN_B2, "y", wb_in, own, a, b, lambda at: in2_sem.at[1, part])

    forward(1)
    send(OUT_A1, "y", lambda k: wout.at[:, 0:half], lambda k: wa_out.at[0, at_y[-k % ny]], wa_out.at[0, 1:])
    send(OUT_B1, "z", lambda k: wout.at[:, half:], lambda k: wb_out.at[0, at_z[-k % nz]], wb_out.at[0, 1:])
    if max(ny, nz) > 2:
        forward(2)

    @pl.when(z != dp)
    def _():
        param_copy(PK_Z, 1, pk_z, pk_z).wait_recv()
        param_copy(AUX_Z, 1, aux_z, aux_z).wait_recv()

    send(PK_Y, "y", lambda k: pk_z, lambda k: pk_y.at[y], pk_y.at[1:])
    send(AUX_Y, "y", lambda k: aux_z, lambda k: aux_y.at[y], aux_y.at[1:])
    pk_y[y] = pk_z[...]
    aux_y[y] = aux_z[...]


    def weights_of(wa, wb, b):
        return weights_at(wa, wb, slot_of(nz, lax.rem(b - z + nz, nz)))

    def weights_at(wa, wb, at):
        place = [slot_of(ny, lax.rem(g - y + ny, ny)) for g in range(ny)]
        left = jnp.concatenate([wa[at, i] for i in place], axis=0)
        right = jnp.concatenate([wb[i, at] for i in place], axis=0)
        return jnp.concatenate([left, right], axis=1)

    def project(phase, act, wa, wb, out, recv):
        for k in ring_order(nd, True):
            j = peer("d", k)
            out[j] = dot(act[...], weights_of(wa, wb, j), NT).astype(BF16)
            copy(phase, "d", j, out.at[j], recv.at[dp]).start()
        sent.append((phase, "d", recv.at[0 : nd - 1]))
        recv[dp] = dot(act[...], weights_of(wa, wb, dp), NT).astype(BF16)

    for load in loads[9:]:
        load.wait()
    for part, (a, e) in enumerate(parts(nz)):
        got = wb_in.at[1:, a:e]
        copy(IN_B2, "y", peer("y", 1), got, got, in2_sem.at[1, part]).wait_recv()
        for at in range(max(a, 1), e):
            copy(IN_A2, "z", peer("z", 1), wa_in.at[at], wa_in.at[at], in2_sem.at[0, at]).wait_recv()
        targets = [peer("z", slots(nz)[0][at]) for at in range(a, e)]
        for at, b in zip(range(a, e), targets):
            d_send[b] = dot(tok[...], weights_at(wa_in, wb_in, at), NT).astype(BF16)

            @pl.when(b != dp)
            def _():
                copy(DRIVE, "d", b, d_send.at[b], d_recv.at[dp]).start()

            @pl.when(b == dp)
            def _():
                d_recv[dp] = d_send[dp]

        if part == 1:
            arrive(OUT_A1, "y", wa_out.at[0, 1:])
            spread(OUT_A2, "z", wa_out, wa_out.at[0, 0:ny], 0, ny)
            arrive(OUT_B1, "z", wb_out.at[0, 1:])
            spread(OUT_B2, "y", wb_out, wb_out.at[0, 0:nz], 0, nz)

    sent.append((IN_A2, "z", wa_in.at[1:]))
    sent.append((IN_B2, "y", wb_in.at[1:]))
    sent.append((DRIVE, "d", d_recv.at[0 : nd - 1]))

    arrive(PK_Y, "y", pk_y.at[0 : ny - 1])
    arrive(AUX_Y, "y", aux_y.at[0 : ny - 1])
    packed = pk_y[...].reshape(own_ch, four)
    diag = lax.div(iota((own_ch, lanes), 0), per_group) == lax.div(iota((own_ch, lanes), 1), states)
    s_row, s_lane = iota((four, lanes), 0), lax.rem(iota((four, lanes), 1), states)
    for at, ref in enumerate((bre, bim, cre, cim)):
        spread = (s_row == s_lane + at * states).astype(F32).astype(BF16)
        ref[...] = jnp.where(diag, dot(packed, spread), 0.0).astype(BF16)
    group_of_lane = lax.div(iota((1, lanes), 1), states)
    group_of_ch = lax.div(iota((1, own_ch), 1), per_group)
    dec = (jnp.zeros((1, lanes), F32), jnp.zeros((1, lanes), F32))
    gain = jnp.zeros((1, own_ch), F32)
    for g in range(ny):
        dec = (
            jnp.where(group_of_lane == g, aux_y[g, 0:1, :], dec[0]),
            jnp.where(group_of_lane == g, aux_y[g, 1:2, :], dec[1]),
        )
        gain = jnp.where(group_of_ch == g, aux_y[g, 2:3, 0:own_ch], gain)
    row = iota((rows, lanes), 0)
    up = (jnp.ones((rows, lanes), F32), jnp.zeros((rows, lanes), F32))
    down = up
    factor = dec
    for k in range(log2(rows)):
        bit = lax.rem(lax.div(row, 1 << k), 2) == 1
        more = cmul(up, factor)
        up = (jnp.where(bit, more[0], up[0]), jnp.where(bit, more[1], up[1]))
        more = cmul(down, factor)
        down = (jnp.where(bit, down[0], more[0]), jnp.where(bit, down[1], more[1]))
        factor = square(factor, 1)
    u_re[...], u_im[...] = up
    v_re[...], v_im[...] = down
    dec_chunk = factor

    def total(recv):
        s = recv[0].astype(F32)
        for b in range(1, nd):
            s = s + recv[b].astype(F32)
        return s.astype(BF16)

    arrive(DRIVE, "d", d_recv.at[0 : nd - 1])
    x = total(d_recv)

    chunks = ny * nz

    def to_all(phase, own, recv, reverse):
        far = lambda k, n: min(k, n - k)
        offsets = [(a, b) for a in range(nz) for b in range(ny) if a or b]
        for a, b in sorted(offsets, key=lambda o: -far(o[0], nz) - far(o[1], ny)):
            j = peer("z", a) * ny + peer("y", b)
            ahead = sp - j if reverse else j - sp
            pltpu.make_async_remote_copy(
                src_ref=own,
                dst_ref=recv.at[lax.rem(ahead - 1 + 2 * chunks, chunks)],
                send_sem=ssem.at[phase],
                recv_sem=rsem.at[phase],
                device_id=(j, dp),
                device_id_type=MESH,
            ).start()
        sent.append((phase, "y", recv.at[1:]))

    def entering(recv, reverse):
        held = iota((chunks, 2, lanes), 0) < (chunks - 1 - sp if reverse else sp)
        state = jnp.where(held, recv[...].astype(F32), 0.0)
        by_re = jnp.sum(state * w_re[...], axis=0)
        by_im = jnp.sum(state * w_im[...], axis=0)
        if reverse:
            by_im = -by_im
        return by_re[0:1] - by_im[1:2], by_re[1:2] + by_im[0:1]

    def summed(pair, table_re, table_im, sign):
        tr, ti = table_re[...], sign * table_im[...]
        re, im = cmul(pair, (tr, ti))
        return jnp.sum(re, axis=0, keepdims=True), jnp.sum(im, axis=0, keepdims=True)

    def put(ref, pair):
        ref[...] = jnp.concatenate(pair, axis=0).astype(ref.dtype)

    push = (dot(x, bre[...]), dot(x, bim[...]))
    final = summed(push, v_re, v_im, 1.0)
    put(f_own, final)
    to_all(FWD_Y, f_own, f_recv, False)
    local = scan_rows(push, dec, False)
    gathered(OUT_A2, "z", wa_out)
    gathered(OUT_B2, "y", wb_out)
    project(BACK, cot, wa_out, wb_out, b_send, b_recv)

    row = iota((chunks, lanes), 0)
    power, factor = (jnp.ones((chunks, lanes), F32), jnp.zeros((chunks, lanes), F32)), dec_chunk
    for k in range(log2(chunks)):
        bit = lax.rem(lax.div(row, 1 << k), 2) == 1
        more = cmul(power, factor)
        power = (jnp.where(bit, more[0], power[0]), jnp.where(bit, more[1], power[1]))
        factor = square(factor, 1)
    w_re[...] = jnp.broadcast_to(power[0][:, None, :], (chunks, 2, lanes))
    w_im[...] = jnp.broadcast_to(power[1][:, None, :], (chunks, 2, lanes))
    arrive(FWD_Y, "y", f_recv.at[1:])
    start = cmul(dec, entering(f_recv, False))
    add = cmul((u_re[...], u_im[...]), start)
    state_re, state_im = (local[0] + add[0]).astype(BF16), (local[1] + add[1]).astype(BF16)
    mixed = dot(state_re, cre[...], NT) - dot(state_im, cim[...], NT) + gain * x.astype(F32)
    c0 = math.sqrt(2.0 / math.pi)
    sq = mixed * mixed
    th = jnp.tanh(c0 * mixed * (1.0 + 0.044715 * sq))
    half_up = 0.5 * (1.0 + th)
    gated = (mixed * half_up).astype(BF16)
    slope = half_up + 0.5 * mixed * (1.0 - th * th) * (c0 * (1.0 + 3.0 * 0.044715 * sq))
    arrive(BACK, "d", b_recv.at[0 : nd - 1])
    inner = slope * total(b_recv).astype(F32)
    inner_b = inner.astype(BF16)
    pulled = (dot(inner_b, cre[...]), -dot(inner_b, cim[...]))
    opening = summed(pulled, u_re, u_im, -1.0)
    put(a_own, opening)
    to_all(BWD_Y, a_own, a_recv, True)
    gat_own[...] = gated
    send(GATED, "d", lambda k: gat_own, lambda k: gat_all.at[dp], gat_all.at[0 : nd - 1])
    gat_all[dp] = gated
    back_dec = conj(dec)
    local = scan_rows(pulled, back_dec, True)
    def block_of_grad(b, cols, act, sa, sb):
        part = dot(cols[b], act[...], TN).astype(BF16)
        sa[b] = part[:, 0:half].reshape(ny, per_group, half)
        sb[:, b] = part[:, half:].reshape(ny, per_group, half)

    def hand_on(phase, phase_h, axis, s, h, r):
        if size[axis] != 8:
            for k in ring_order(size[axis], True):
                copy(phase, axis, peer(axis, k), s.at[peer(axis, k)], r.at[slot[axis](-k)]).start()
            sent.append((phase, axis, r.at[1:]))
        else:
            copy(phase_h, axis, peer(axis, 2 + 4 * core), s.at[peer(axis, 4)], h.at[2]).start()
            copy(phase_h, axis, peer(axis, 1), s.at[peer(axis, 3)], h.at[0]).start()
            copy(phase_h, axis, peer(axis, 7), s.at[peer(axis, 5)], h.at[1]).start()
            copy(phase, axis, peer(axis, 1), s.at[peer(axis, 1)], r.at[1]).start()
            copy(phase, axis, peer(axis, 7), s.at[peer(axis, 7)], r.at[2]).start()
        r[0] = s[here[axis]]

    def add_to(s, j, part):
        s[j] = (s[j].astype(F32) + part.astype(F32)).astype(BF16)

    def pass_on(phase, phase_h, axis, s, h, r):
        if size[axis] == 8:
            arrive(phase_h, axis, h)
            add_to(s, peer(axis, 2), h[0])
            add_to(s, peer(axis, 6), h[1])
            add_to(s, peer(axis, 2 + 4 * core), h[2])
            copy(phase, axis, peer(axis, 2), s.at[peer(axis, 2)], r.at[3]).start()
            copy(phase, axis, peer(axis, 6), s.at[peer(axis, 6)], r.at[4]).start()
            sent.append((phase_h, axis, h))
            sent.append((phase, axis, r.at[1:]))

    def reduced(recv, n):
        s = recv[0].astype(F32)
        for j in range(1, n):
            s = s + recv[j].astype(F32)
        return s

    def second_step(phase_a1, phase_b1, phase_a2, phase_b2, ra, rb, s2a, s2b, r2a, r2b):
        arrive(phase_a1, "z", ra.at[1:])
        s2a[...] = reduced(ra, ra.shape[0]).astype(BF16)
        send(phase_a2, "y", lambda k: s2a.at[peer("y", k)], lambda k: r2a.at[at_y[-k % ny]], r2a.at[1:])
        r2a[0] = s2a[y]
        arrive(phase_b1, "y", rb.at[1:])
        s2b[...] = reduced(rb, rb.shape[0]).astype(BF16)
        send(phase_b2, "z", lambda k: s2b.at[peer("z", k)], lambda k: r2b.at[at_z[-k % nz]], r2b.at[1:])
        r2b[0] = s2b[z]

    scale = (rows * ny * nz) ** -0.5

    def finish(phase_a2, phase_b2, r2a, r2b, out):
        arrive(phase_a2, "y", r2a.at[0 : ny - 1])
        arrive(phase_b2, "z", r2b.at[0 : nz - 1])
        out[:, 0:half] = reduced(r2a, ny) * scale
        out[:, half:] = reduced(r2b, nz) * scale

    arrive(GATED, "d", gat_all.at[0 : nd - 1])
    for b in range(nd):
        block_of_grad(b, gat_all, cot, go_sa, go_sb)
    hand_on(GO_A1, GO_HA, "z", go_sa, go_ha, go_ra)
    hand_on(GO_B1, GO_HB, "y", go_sb, go_hb, go_rb)

    arrive(BWD_Y, "y", a_recv.at[1:])
    start = cmul(back_dec, entering(a_recv, True))
    add = cmul((v_re[...], -v_im[...]), start)
    adj_re, adj_im = (local[0] + add[0]).astype(BF16), (local[1] + add[1]).astype(BF16)
    mix = (dot(adj_re, bre[...], NT) + dot(adj_im, bim[...], NT) + gain * inner).astype(BF16)
    mix_own[...] = mix
    send(MIX, "d", lambda k: mix_own, lambda k: mix_all.at[dp], mix_all.at[0 : nd - 1], lambda k: mix_sem.at[k])
    mix_all[dp] = mix

    block_of_grad(dp, mix_all, tok, gi_sa, gi_sb)
    order = ring_order(nd, False)
    for batch in (order[0:1], order[1:2], order[2:]):
        for k in batch:
            j = peer("d", nd - k)
            copy(MIX, "d", j, mix_own, mix_all.at[j], mix_sem.at[k]).wait_recv()
        for k in batch:
            block_of_grad(peer("d", nd - k), mix_all, tok, gi_sa, gi_sb)
    hand_on(GI_A1, GI_HA, "z", gi_sa, gi_ha, gi_ra)
    hand_on(GI_B1, GI_HB, "y", gi_sb, gi_hb, gi_rb)
    pass_on(GO_A1, GO_HA, "z", go_sa, go_ha, go_ra)
    pass_on(GO_B1, GO_HB, "y", go_sb, go_hb, go_rb)
    grad = dot(mix_all[0], weights_of(wa_in, wb_in, 0))
    for b in range(1, nd):
        grad = grad + dot(mix_all[b], weights_of(wa_in, wb_in, b))
    o_tok[...] = grad.astype(BF16)
    pass_on(GI_A1, GI_HA, "z", gi_sa, gi_ha, gi_ra)
    pass_on(GI_B1, GI_HB, "y", gi_sb, gi_hb, gi_rb)
    second_step(GO_A1, GO_B1, GO_A2, GO_B2, go_ra, go_rb, go_s2a, go_s2b, go_r2a, go_r2b)
    second_step(GI_A1, GI_B1, GI_A2, GI_B2, gi_ra, gi_rb, gi_s2a, gi_s2b, gi_r2a, gi_r2b)
    finish(GO_A2, GO_B2, go_r2a, go_r2b, o_out)
    finish(GI_A2, GI_B2, gi_r2a, gi_r2b, o_in)

    @pl.when(z == dp)
    def _():
        param_copy(PK_Z, 1, pk_y.at[0 : nz - 1], pk_y.at[0 : nz - 1]).wait_send()
        param_copy(AUX_Z, 1, aux_y.at[0 : nz - 1], aux_y.at[0 : nz - 1]).wait_send()

    for phase, axis, whole in sent:
        copy(phase, axis, peer(axis, 1), whole, whole).wait_send()


def store(a, b, c, out_a, out_b, out_c, sem):
    copies = [pltpu.make_async_copy(s, d, sem.at[i]) for i, (s, d) in enumerate(((a, out_a), (b, out_b), (c, out_c)))]
    for copy in copies:
        copy.start()
    for copy in copies:
        copy.wait()


def on_device(ny, nz, nd, tok, cot, win, wout, rate, freq, slog, dr, di, rr, ri, skip):
    rows, cols = tok.shape
    half = cols // 2
    states, c = rate.shape[1], skip.shape[1]
    own_ch, lanes, four = ny * c, ny * states, 4 * states
    V = pltpu.VMEM
    come = lambda n: 5 if n == 8 else n
    relayed = [
        V((nz, ny, c, half), BF16), V((ny, nz, c, half), BF16),
        V((3, ny, c, half), BF16), V((3, nz, c, half), BF16),
        V((come(nz), ny, c, half), BF16), V((come(ny), nz, c, half), BF16),
        V((ny, c, half), BF16), V((nz, c, half), BF16),
        V((ny, c, half), BF16), V((nz, c, half), BF16),
    ]
    vm = pl.BlockSpec(memory_space=pltpu.VMEM)
    drive = [jnp.swapaxes(a, 1, 2) for a in (dr, di)]
    args = (tok, cot, win, wout, rate, freq, *drive, rr, ri, skip)
    outs = pl.pallas_call(
        functools.partial(kernel, ny, nz, nd),
        out_shape=(
            jax.ShapeDtypeStruct((rows, cols), BF16),
            jax.ShapeDtypeStruct(win.shape, F32),
            jax.ShapeDtypeStruct(wout.shape, F32),
        ),
        in_specs=[pl.BlockSpec(memory_space=pltpu.SMEM)] + [pl.BlockSpec(memory_space=pltpu.HBM)] * len(args),
        out_specs=(vm, vm, vm),
        scratch_shapes=[
            *[V(a.shape, a.dtype) for a in args],
            V((c, four), BF16), V((8, lanes), F32),
            V((c, four), BF16), V((8, lanes), F32),
            V((ny, c, four), BF16), V((ny, 8, lanes), F32),
            V((nz, ny, c, half), BF16), V((ny, nz, c, half), BF16),
            V((nz, ny, c, half), BF16), V((ny, nz, c, half), BF16),
            V((nd, rows, own_ch), BF16), V((nd, rows, own_ch), BF16),
            V((nd, rows, own_ch), BF16), V((nd, rows, own_ch), BF16),
            V((2, lanes), BF16), V((ny * nz, 2, lanes), BF16),
            V((2, lanes), BF16), V((ny * nz, 2, lanes), BF16),
            V((ny * nz, 2, lanes), F32), V((ny * nz, 2, lanes), F32),
            V((rows, own_ch), BF16), V((nd, rows, own_ch), BF16),
            V((rows, own_ch), BF16), V((nd, rows, own_ch), BF16),
            *relayed, *relayed,
            *[V((own_ch, lanes), BF16)] * 4,
            *[V((rows, lanes), F32)] * 4,
            pltpu.SemaphoreType.DMA((PHASES,)),
            pltpu.SemaphoreType.DMA((PHASES,)),
            pltpu.SemaphoreType.DMA((2, 3)),
            pltpu.SemaphoreType.DMA((2, 8)),
            pltpu.SemaphoreType.DMA((nd,)),
            pltpu.SemaphoreType.DMA((len(args),)),
        ],
        compiler_params=pltpu.CompilerParams(
            collective_id=0, has_side_effects=True, vmem_limit_bytes=48 * 1024 * 1024
        ),
        name="mixer",
    )(slog, *[pltpu.with_memory_space_constraint(a, pltpu.HBM) for a in args])
    return pl.pallas_call(
        store,
        out_shape=tuple(jax.ShapeDtypeStruct(o.shape, o.dtype) for o in outs),
        in_specs=[vm] * 3,
        out_specs=(pl.BlockSpec(memory_space=pltpu.HBM),) * 3,
        scratch_shapes=[pltpu.SemaphoreType.DMA((3,))],
        compiler_params=pltpu.CompilerParams(vmem_limit_bytes=8 * 1024 * 1024),
        name="store",
    )(*outs)


def solution(mesh):
    nd = mesh.shape["dp"]
    nz = nd
    ny = mesh.shape["sp"] // nz
    return jax.shard_map(
        functools.partial(on_device, ny, nz, nd),
        mesh=mesh,
        in_specs=(
            P("sp", "dp"), P("sp", "dp"), P("sp", "dp"), P("sp", "dp"),
            P("sp", None), P("sp", None), P("sp"),
            P("sp", None, None), P("sp", None, None), P("sp", None, None), P("sp", None, None),
            P("sp", None),
        ),
        out_specs=(P("sp", "dp"), P("sp", "dp"), P("sp", "dp")),
        check_vma=False,
    )
```
